32 devices in a mesh: sp: 8 (over z, x), tp: 4 (over y, core).
Axes of the slice: x: 2, y: 2, z: 4, core: 2. Of those that a mesh axis runs over, the one named last changes fastest.
Arguments:
- query_wide: bfloat16 [1024, 1536], P('sp', 'tp'), may hold values from -600 to 600
- query_narrow: bfloat16 [1024, 1024], P('sp', 'tp'), may hold values from -600 to 600
- latent: bfloat16 [1024, 512], P('sp'), may hold values from -6 to 6
- rope_key: bfloat16 [1024, 64], P('sp'), may hold values from -6 to 6
- latent_norm_weight: float32 [512], replicated, may hold values from 0.1 to 1.9
- broad_key_lift: bfloat16 [512, 1024], P(None, 'tp'), may hold values from -0.25 to 0.25
- broad_value_lift: bfloat16 [512, 1024], P(None, 'tp'), may hold values from -0.25 to 0.25
- slim_key_lift: bfloat16 [512, 512], P(None, 'tp'), may hold values from -0.25 to 0.25
- slim_value_lift: bfloat16 [512, 512], P(None, 'tp'), may hold values from -0.25 to 0.25
- out_wide: bfloat16 [1024, 2048], P('tp'), may hold values from -0.4375 to 0.4375
- out_narrow: bfloat16 [512, 2048], P('tp'), may hold values from -0.4375 to 0.4375
- resid: bfloat16 [1024, 2048], P('sp'), may hold values from -20 to 20
- ffn_gain: float32 [2048], replicated, may hold values from 0.1 to 1.9
- group_route: int32 [1024], P('sp'), may hold values from 0 to 7, as said below
- expert_pair: int32 [1024, 2], P('sp'), may hold values from 0 to 3, all different within a row
- group_prob: float32 [1024], P('sp'), may hold values from 0.2 to 1
- expert_prob: float32 [1024, 2], P('sp'), may hold values from 0.05 to 1
- gate_weight: bfloat16 [8, 4, 2048, 512], P('sp', None, None, 'tp'), may hold values from -0.125 to 0.125
- up_weight: bfloat16 [8, 4, 2048, 512], P('sp', None, None, 'tp'), may hold values from -0.125 to 0.125
- down_weight: bfloat16 [8, 4, 512, 2048], P('sp', None, 'tp'), may hold values from -0.25 to 0.25
Outputs:
- mixed: bfloat16 [1024, 2048], P('sp', 'tp')
The draws below stay inside these ranges and needn't reach their ends.
Inputs may be any that keep to these rules, and one draw needn't show every extreme that they name: `group_route`: of the 128 tokens of one index of sp at most 32 name one group; in every draw one group is named by exactly 32 tokens of every index of sp, and every index of sp names one more group exactly 32 times. `expert_pair`: A token's two experts are different.
All inputs are finite; a program needn't handle non-finite values.
Results may differ from the reference program's by a relative error of at most 0.017.
Values may be sent and summed in bfloat16 or wider, within the bound.
No kernel may reach another device: no remote copies, remote signals or barrier semaphores. Data moves between devices by JAX's collectives and lax.ppermute only.
A program may use at most 128 MiB of HBM per device.

```python
import math
import jax
import jax.numpy as jnp
from jax import lax

D = 2048
WIDE_HEADS = 8
SLIM_HEADS = 8
PLAIN_WIDTH_WIDE = 128
PLAIN_WIDTH_SLIM = 64
ROPE = 64
VALUE_WIDTH_WIDE = 128
VALUE_WIDTH_SLIM = 64
LATENT_RANK = 512
EPG = 4
FF = 512
TOK_DEV = 128
TOKEN_COUNT = 1024
GROUPS = 8
CAP = 32
N_SP = 8
N_TP = 4


def query_draw(key, columns):
    base_values = 2.5 * jax.random.truncated_normal(key, -6.0, 6.0, (TOKEN_COUNT, columns), jnp.float32)
    return base_values.astype(jnp.bfloat16)


def draw_query_wide(key, part):
    return query_draw(jax.random.fold_in(key, 3), WIDE_HEADS * (PLAIN_WIDTH_WIDE + ROPE))


def draw_query_narrow(key, part):
    return query_draw(jax.random.fold_in(key, 5), SLIM_HEADS * (PLAIN_WIDTH_SLIM + ROPE))


def draw_resid(key, part):
    column = jnp.arange(D).astype(jnp.float32)
    column_scale = 0.3 * 9.0 ** (column / (D - 1))
    base_values = jax.random.truncated_normal(jax.random.fold_in(key, 19), -6.0, 6.0, (TOKEN_COUNT, D), jnp.float32)
    return (base_values * column_scale[None, :]).astype(jnp.bfloat16)


def draw_group_route(key, part):
    heavy_all = jax.random.randint(jax.random.fold_in(key, 11), (), 0, GROUPS)
    slot_group = (jnp.arange(GROUPS * CAP) // CAP).astype(jnp.int32)

    def one_device(device_index):
        device_key = jax.random.fold_in(jax.random.fold_in(key, 13), device_index)
        first_key, second_key, third_key = jax.random.split(device_key, 3)
        second_group = (heavy_all + 1 + jax.random.randint(first_key, (), 0, GROUPS - 1)) % GROUPS
        shuffled = jax.random.permutation(second_key, GROUPS * CAP)
        position = jnp.zeros((GROUPS * CAP,), jnp.int32).at[shuffled].set(jnp.arange(GROUPS * CAP, dtype=jnp.int32))
        heavy_slot = (slot_group == heavy_all) | (slot_group == second_group)
        sort_score = jnp.where(heavy_slot, jnp.arange(GROUPS * CAP, dtype=jnp.int32), GROUPS * CAP + position)
        picked = slot_group[jnp.argsort(sort_score, stable=True)][:TOK_DEV]
        return picked[jax.random.permutation(third_key, TOK_DEV)]
    return jax.vmap(one_device)(jnp.arange(GROUPS)).reshape(TOKEN_COUNT).astype(jnp.int32)


def level_of(own_key, dims, cuts, low, high):
    gain = 1.0
    for axis_at, blocks in cuts:
        steps = jax.random.uniform(jax.random.fold_in(jax.random.fold_in(own_key, 6), axis_at), (blocks,), jnp.float32, low / len(cuts), high / len(cuts))
        gain = gain * jnp.repeat(jnp.exp(steps), dims[axis_at] // blocks).reshape((-1,) + (1,) * (len(dims) - 1 - axis_at))
    return gain


def choose_distinct(own_key, rows, number_of, top, lift):
    sequence = jax.random.permutation(jax.random.fold_in(own_key, 1), number_of)
    favour = sequence
    for power in range(3):
        favour = favour * favour // number_of
    favour = favour * lift // number_of
    lots = jax.random.randint(jax.random.fold_in(own_key, 2), (rows, number_of), 0, 4096) + favour
    holders = jax.random.permutation(jax.random.fold_in(own_key, 3), rows)[jnp.arange(number_of) % rows]
    lots = jnp.where(jnp.arange(rows)[:, None] == holders[None, :], 1 << 14, lots)
    priority = lots * number_of + jnp.arange(number_of)
    return lax.top_k(priority.astype(jnp.int32), top)[1].astype(jnp.int32)


def noise(rng, extent, scale, bound, pieces=(), held_as=jnp.bfloat16):
    factor_of = level_of(rng, extent, pieces, -0.22, 0.18) if pieces else 1.0
    result = jax.random.normal(rng, extent, jnp.float32) * scale * factor_of
    return jnp.minimum(jnp.maximum(result, -bound), bound).astype(held_as)


def setup_inputs(seed: int = 0) -> dict:
    seeds = jax.random.split(jax.random.key(seed), 21)
    return {
        "query_wide": draw_query_wide(jax.random.fold_in(seeds[20], 71), 0),
        "query_narrow": draw_query_narrow(jax.random.fold_in(seeds[20], 71), 0),
        "latent": noise(seeds[2], (TOKEN_COUNT, LATENT_RANK), 1.0, 6.0, ((0, 8),)),
        "rope_key": noise(seeds[3], (TOKEN_COUNT, ROPE), 1.0, 6.0, ((0, 8),)),
        "latent_norm_weight": jnp.clip(1.0 + 0.18 * jax.random.normal(seeds[4], (LATENT_RANK,), jnp.float32), 0.1, 1.9),
        "broad_key_lift": noise(seeds[5], (LATENT_RANK, WIDE_HEADS * PLAIN_WIDTH_WIDE), LATENT_RANK ** -0.5, 0.25, ((1, 4),)),
        "broad_value_lift": noise(seeds[6], (LATENT_RANK, WIDE_HEADS * VALUE_WIDTH_WIDE), LATENT_RANK ** -0.5, 0.25, ((1, 4),)),
        "slim_key_lift": noise(seeds[7], (LATENT_RANK, SLIM_HEADS * PLAIN_WIDTH_SLIM), LATENT_RANK ** -0.5, 0.25, ((1, 4),)),
        "slim_value_lift": noise(seeds[8], (LATENT_RANK, SLIM_HEADS * VALUE_WIDTH_SLIM), LATENT_RANK ** -0.5, 0.25, ((1, 4),)),
        "out_wide": noise(seeds[9], (WIDE_HEADS * VALUE_WIDTH_WIDE, D), ((WIDE_HEADS * VALUE_WIDTH_WIDE + SLIM_HEADS * VALUE_WIDTH_SLIM) // 9) ** -0.5, 0.4375, ((0, 4),)),
        "out_narrow": noise(seeds[10], (SLIM_HEADS * VALUE_WIDTH_SLIM, D), ((WIDE_HEADS * VALUE_WIDTH_WIDE + SLIM_HEADS * VALUE_WIDTH_SLIM) // 9) ** -0.5, 0.4375, ((0, 4),)),
        "resid": draw_resid(jax.random.fold_in(seeds[20], 71), 0),
        "ffn_gain": jnp.clip(1.0 + 0.18 * jax.random.normal(seeds[12], (D,), jnp.float32), 0.1, 1.9),
        "group_route": draw_group_route(jax.random.fold_in(seeds[20], 71), 0),
        "expert_pair": choose_distinct(seeds[14], TOKEN_COUNT, EPG, 2, 0),
        "group_prob": jnp.clip(0.2 + 0.8 * jax.random.uniform(seeds[15], (TOKEN_COUNT,), jnp.float32) ** level_of(seeds[15], (TOKEN_COUNT,), ((0, 8),), -0.2, 0.2), 0.2, 1.0),
        "expert_prob": jnp.clip(jnp.exp(math.log(1.0) - 2.9957323 * jax.random.uniform(seeds[16], (TOKEN_COUNT, 2), jnp.float32) ** level_of(seeds[16], (TOKEN_COUNT, 2), ((0, 8),), -0.2, 0.2)), 0.05, 1.0),
        "gate_weight": noise(seeds[17], (GROUPS, EPG, D, FF), D ** -0.5, 0.125, ((0, 8), (3, 4))),
        "up_weight": noise(seeds[18], (GROUPS, EPG, D, FF), D ** -0.5, 0.125, ((0, 8), (3, 4))),
        "down_weight": noise(seeds[19], (GROUPS, EPG, FF, D), FF ** -0.5, 0.25, ((0, 8), (2, 4))),
    }


ROPE_BASE = 10000.0
EPSILON = 1e-06

def rms_scale(values, gain_row):
    widened = values.astype(jnp.float32)
    return widened * lax.rsqrt(lax.optimization_barrier(jnp.mean(widened * widened, axis=-1, keepdims=True)) + EPSILON) * gain_row.astype(jnp.float32)

def angles(positions, width):
    frequency = 1.0 / ROPE_BASE ** (jnp.arange(0, width, 2).astype(jnp.float32) / width)
    return positions.astype(jnp.float32)[:, None] * frequency[None, :]

def rotary(values, angle_table):
    half_width = values.shape[-1] // 2
    first_half = values[..., :half_width]
    second = values[..., half_width:]
    return jnp.concatenate([first_half * jnp.cos(angle_table) - second * jnp.sin(angle_table), second * jnp.cos(angle_table) + first_half * jnp.sin(angle_table)], axis=-1)

def stored(values):
    return lax.optimization_barrier(values.astype(jnp.bfloat16)).astype(jnp.float32)

def attention(query_nope, query_rot, key_nope, key_rot, value_rows, scale):
    key_pos = jnp.arange(TOKEN_COUNT).astype(jnp.int32)

    def one_block(block_index):
        first_row = (block_index * TOK_DEV).astype(jnp.int32)
        nope_rows = lax.dynamic_slice_in_dim(query_nope, first_row, TOK_DEV, 0)
        rot_rows = lax.dynamic_slice_in_dim(query_rot, first_row, TOK_DEV, 0)
        scores = jnp.einsum('thd,khd->htk', nope_rows, key_nope) + jnp.einsum('thd,kd->htk', rot_rows, key_rot)
        scores = scores * scale
        query_pos = first_row + jnp.arange(TOK_DEV).astype(jnp.int32)
        scores = jnp.where((query_pos[:, None] >= key_pos[None, :])[None], scores, -jnp.inf)
        row_peak = lax.optimization_barrier(jnp.max(scores, axis=-1, keepdims=True))
        weights = jnp.exp(scores - row_peak)
        row_total = lax.optimization_barrier(jnp.sum(weights, axis=-1))
        mixed_rows = jnp.einsum('htk,khd->thd', stored(weights), value_rows)
        return (mixed_rows / row_total.T[:, :, None]).astype(jnp.bfloat16)
    blocks = lax.map(one_block, jnp.arange(TOKEN_COUNT // TOK_DEV).astype(jnp.int32))
    return blocks.reshape(TOKEN_COUNT, -1)

def reference(query_wide, query_narrow, latent, rope_key, latent_norm_weight, broad_key_lift, broad_value_lift, slim_key_lift, slim_value_lift, out_wide, out_narrow, resid, ffn_gain, group_route, expert_pair, group_prob, expert_prob, gate_weight, up_weight, down_weight):
    angle_table = angles(jnp.arange(TOKEN_COUNT).astype(jnp.int32), ROPE)
    latent_rows = rms_scale(latent, latent_norm_weight).astype(jnp.bfloat16)
    key_rot = stored(rotary(rope_key.astype(jnp.float32), angle_table))
    key_wide = stored(jnp.dot(latent_rows, broad_key_lift, preferred_element_type=jnp.float32)).reshape(TOKEN_COUNT, WIDE_HEADS, PLAIN_WIDTH_WIDE)
    value_wide = stored(jnp.dot(latent_rows, broad_value_lift, preferred_element_type=jnp.float32)).reshape(TOKEN_COUNT, WIDE_HEADS, VALUE_WIDTH_WIDE)
    key_narrow = stored(jnp.dot(latent_rows, slim_key_lift, preferred_element_type=jnp.float32)).reshape(TOKEN_COUNT, SLIM_HEADS, PLAIN_WIDTH_SLIM)
    value_narrow = stored(jnp.dot(latent_rows, slim_value_lift, preferred_element_type=jnp.float32)).reshape(TOKEN_COUNT, SLIM_HEADS, VALUE_WIDTH_SLIM)
    wide_rows = query_wide.reshape(TOKEN_COUNT, WIDE_HEADS, PLAIN_WIDTH_WIDE + ROPE).astype(jnp.float32)
    wide_rot = stored(rotary(wide_rows[..., PLAIN_WIDTH_WIDE:], angle_table[:, None, :]))
    narrow_rows = query_narrow.reshape(TOKEN_COUNT, SLIM_HEADS, PLAIN_WIDTH_SLIM + ROPE).astype(jnp.float32)
    narrow_rot = stored(rotary(narrow_rows[..., PLAIN_WIDTH_SLIM:], angle_table[:, None, :]))
    att_wide = attention(wide_rows[..., :PLAIN_WIDTH_WIDE], wide_rot, key_wide, key_rot, value_wide, (PLAIN_WIDTH_WIDE + ROPE) ** (-0.5))
    att_narrow = attention(narrow_rows[..., :PLAIN_WIDTH_SLIM], narrow_rot, key_narrow, key_rot, value_narrow, (PLAIN_WIDTH_SLIM + ROPE) ** (-0.5))
    wide_share = WIDE_HEADS // N_TP * VALUE_WIDTH_WIDE
    narrow_share = SLIM_HEADS // N_TP * VALUE_WIDTH_SLIM
    projected = jnp.zeros((TOKEN_COUNT, D), jnp.float32)
    for part_index in range(N_TP):
        wide_lo = part_index * wide_share
        narrow_lo = part_index * narrow_share
        partial_value = jnp.dot(att_wide[:, wide_lo:wide_lo + wide_share], out_wide[wide_lo:wide_lo + wide_share], preferred_element_type=jnp.float32)
        partial_value = partial_value + jnp.dot(att_narrow[:, narrow_lo:narrow_lo + narrow_share], out_narrow[narrow_lo:narrow_lo + narrow_share], preferred_element_type=jnp.float32)
        projected = projected + stored(partial_value)
    stream = (resid.astype(jnp.float32) + projected).astype(jnp.bfloat16)
    normed = rms_scale(stream, ffn_gain).astype(jnp.bfloat16)
    share_of = group_prob[:, None] * expert_prob / lax.optimization_barrier(jnp.sum(expert_prob, axis=1, keepdims=True))
    chosen = (expert_pair[:, :, None] == jnp.arange(EPG).astype(jnp.int32)[None, None, :]).astype(jnp.float32)
    combine = lax.optimization_barrier(jnp.sum(share_of[:, :, None] * chosen, axis=1)).astype(jnp.bfloat16)
    slot_count = N_SP * CAP
    member = (group_route[:, None] == jnp.arange(GROUPS).astype(jnp.int32)[None, :]).astype(jnp.int32)
    group_rank = lax.optimization_barrier(jnp.sum(jnp.cumsum(member, axis=0) * member, axis=1)) - 1
    slot_index = (group_route * slot_count + group_rank).astype(jnp.int32)
    routed_rows = jnp.zeros((GROUPS * slot_count, D), jnp.bfloat16).at[slot_index].set(normed)
    routed_weights = jnp.zeros((GROUPS * slot_count, EPG), jnp.bfloat16).at[slot_index].set(combine)

    def one_group(operands):
        group_rows, group_weights, gate_group, up_group, down_group = operands
        flat_rows = stored(group_rows)
        gate_act = jnp.einsum('rd,edf->ref', flat_rows, gate_group.astype(jnp.float32))
        up_act = jnp.einsum('rd,edf->ref', flat_rows, up_group.astype(jnp.float32))
        hidden = stored(jax.nn.silu(gate_act) * up_act * group_weights.astype(jnp.float32)[:, :, None])
        hidden = hidden.reshape(slot_count, EPG, N_TP, FF // N_TP)
        down_split = down_group.astype(jnp.float32).reshape(EPG, N_TP, FF // N_TP, D)
        partials = stored(jnp.einsum('repf,epfd->prd', hidden, down_split))
        return lax.optimization_barrier(jnp.sum(partials, axis=0)).astype(jnp.bfloat16)
    results = lax.map(one_group, (routed_rows.reshape(GROUPS, slot_count, D), routed_weights.reshape(GROUPS, slot_count, EPG), gate_weight, up_weight, down_weight))
    moe = results.reshape(GROUPS * slot_count, D)[slot_index]
    return (stream.astype(jnp.float32) + moe.astype(jnp.float32)).astype(jnp.bfloat16)
```

```python
import jax
import jax.numpy as jnp
from jax import lax
from jax.experimental import pallas as pl
from jax.experimental.pallas import tpu as pltpu
from jax.sharding import PartitionSpec as P

PLAIN_WIDTH_WIDE = 128
PLAIN_WIDTH_SLIM = 64
ROPE = 64
VALUE_WIDTH_WIDE = 128
VALUE_WIDTH_SLIM = 64
EPG = 4
LANES = 128

ROPE_BASE = 10000.0
EPSILON = 1e-06
MASKED = -1e30

VMEM = pl.BlockSpec(memory_space=pltpu.VMEM)
SMEM = pl.BlockSpec(memory_space=pltpu.SMEM)


def angles(positions, width):
    frequency = 1.0 / ROPE_BASE ** (jnp.arange(0, width, 2).astype(jnp.float32) / width)
    return positions.astype(jnp.float32)[:, None] * frequency[None, :]


def turn(values, cosine, sine):
    half_width = values.shape[-1] // 2
    first_half = values[..., :half_width]
    second = values[..., half_width:]
    return jnp.concatenate(
        [first_half * cosine - second * sine, second * cosine + first_half * sine], axis=-1
    )


def exchange(values, axis, mask):
    size = lax.axis_size(axis)
    return lax.ppermute(values, axis, [(i, i ^ mask) for i in range(size)])


def pack_kernel(latent_ref, rope_ref, gain_ref, cos_ref, sin_ref, meta_ref, out_ref):
    rank = latent_ref.shape[1]
    widened = latent_ref[...].astype(jnp.float32)
    scale = lax.rsqrt(jnp.mean(widened * widened, axis=-1, keepdims=True) + EPSILON)
    out_ref[:, :rank] = (widened * scale * gain_ref[...]).astype(jnp.bfloat16)
    turned = turn(rope_ref[...].astype(jnp.float32), cos_ref[...], sin_ref[...])
    out_ref[:, rank:] = jnp.concatenate([turned, meta_ref[...]], axis=-1).astype(jnp.bfloat16)


def dot_t(a, b):
    return lax.dot_general(a, b, (((1,), (1,)), ((), ())), preferred_element_type=jnp.float32)


def dot(a, b):
    return jnp.dot(a, b, preferred_element_type=jnp.float32)


def attend_body(where_ref, q_ref, mine_ref, other_ref, kw_ref, vw_ref, kn_ref, vn_ref, state, x_bit):
    heads_w = kw_ref.shape[1] // PLAIN_WIDTH_WIDE
    heads_n = kn_ref.shape[1] // PLAIN_WIDTH_SLIM
    blocks, half, width = mine_ref.shape
    tokens = q_ref.shape[1]
    rank = kw_ref.shape[0]
    place = where_ref[0]
    core = where_ref[1]
    step_blocks = min(blocks, 4)
    rows = step_blocks * half
    shift = half.bit_length() - 1
    for start in range(0, blocks, step_blocks):
        lat = jnp.concatenate(
            [
                mine_ref[start : start + step_blocks].reshape(rows, width),
                other_ref[start : start + step_blocks].reshape(rows, width),
            ],
            axis=0,
        )
        flat = lat[:, :rank]
        rot = lat[:, rank:]
        key_w = dot(flat, kw_ref[...]).astype(jnp.bfloat16)
        key_n = dot(flat, kn_ref[...]).astype(jnp.bfloat16)
        val_w = dot(flat, vw_ref[...]).astype(jnp.bfloat16)
        val_n = dot(flat, vn_ref[...]).astype(jnp.bfloat16)
        lane = lax.broadcasted_iota(jnp.int32, (tokens, 2 * rows), 1)
        row = lax.broadcasted_iota(jnp.int32, (tokens, 2 * rows), 0)
        first = lane < rows
        inner = jnp.where(first, lane, lane - rows)
        block = place ^ (2 * (start + (inner >> shift)) + x_bit)
        offset = jnp.where(first, core, 1 - core)
        key_pos = (block * 2 + offset) * half + (inner & (half - 1))
        visible = row + place * tokens >= key_pos
        new_state = []
        for h in range(heads_w + heads_n):
            if h < heads_w:
                keys = key_w[:, h * PLAIN_WIDTH_WIDE : (h + 1) * PLAIN_WIDTH_WIDE]
                values = val_w[:, h * VALUE_WIDTH_WIDE : (h + 1) * VALUE_WIDTH_WIDE]
                scale = (PLAIN_WIDTH_WIDE + ROPE) ** (-0.5)
            else:
                keys = key_n
                values = val_n
                scale = (PLAIN_WIDTH_SLIM + ROPE) ** (-0.5)
            scores = dot_t(q_ref[h], jnp.concatenate([keys, rot], axis=1)) * scale
            scores = jnp.where(visible, scores, MASKED)
            peak = jnp.max(scores, axis=-1, keepdims=True)
            if state is not None:
                peak = jnp.maximum(peak, state[h][0])
            weights = jnp.exp(scores - peak)
            total = jnp.sum(weights, axis=-1, keepdims=True)
            acc = dot(weights.astype(jnp.bfloat16), values)
            if state is not None:
                keep = jnp.exp(state[h][0] - peak)
                total = total + state[h][1] * keep
                acc = acc + state[h][2] * keep
            new_state.append((peak, total, acc))
        state = new_state
    return state


def first_kernel(where_ref, q_ref, mine_ref, other_ref, kw_ref, vw_ref, kn_ref, vn_ref, peak_ref, total_ref, acc_ref):
    state = attend_body(where_ref, q_ref, mine_ref, other_ref, kw_ref, vw_ref, kn_ref, vn_ref, None, 0)
    for h, (peak, total, acc) in enumerate(state):
        peak_ref[h] = jnp.broadcast_to(peak, peak_ref.shape[1:])
        total_ref[h] = jnp.broadcast_to(total, total_ref.shape[1:])
        acc_ref[h] = acc


def second_kernel(
    where_ref, q_ref, mine_ref, other_ref, kw_ref, vw_ref, kn_ref, vn_ref,
    peak_ref, total_ref, acc_ref, ow_ref, on_ref, keep_ref, send_ref,
):
    heads = peak_ref.shape[0]
    heads_w = kw_ref.shape[1] // PLAIN_WIDTH_WIDE
    state = [(peak_ref[h, :, :1], total_ref[h, :, :1], acc_ref[h]) for h in range(heads)]
    state = attend_body(where_ref, q_ref, mine_ref, other_ref, kw_ref, vw_ref, kn_ref, vn_ref, state, 1)
    done = [acc / total for _, total, acc in state]
    att_w = jnp.concatenate(done[:heads_w], axis=1).astype(jnp.bfloat16)
    att_n = jnp.concatenate(
        [
            done[heads_w + h][:, h * VALUE_WIDTH_SLIM : (h + 1) * VALUE_WIDTH_SLIM]
            for h in range(heads - heads_w)
        ],
        axis=1,
    ).astype(jnp.bfloat16)
    core = where_ref[1]
    pieces, _, quarter = keep_ref.shape
    for piece in range(pieces):
        for ref, bit in ((send_ref, 1 - core), (keep_ref, core)):
            cols = pl.ds(pl.multiple_of((2 * piece + bit) * quarter, LANES), quarter)
            ref[piece] = (dot(att_w, ow_ref[:, cols]) + dot(att_n, on_ref[:, cols])).astype(jnp.bfloat16)


def call(kernel, out_shape, n_args, smem=True, flops=0):
    return pl.pallas_call(
        kernel,
        out_shape=out_shape,
        in_specs=([SMEM] if smem else []) + [VMEM] * (n_args - smem),
        out_specs=jax.tree.map(lambda _: VMEM, out_shape),
        cost_estimate=pl.CostEstimate(flops=flops, transcendentals=0, bytes_accessed=0),
        compiler_params=pltpu.CompilerParams(vmem_limit_bytes=56 * 2**20),
    )


def sum_scatter(low, high, first_bit, place):
    size = lax.axis_size("tp")
    bit = first_bit
    while True:
        mine = ((place >> bit) & 1) == 1
        send = jnp.stack([jnp.where(mine, a, b) for a, b in zip(low, high)]).astype(jnp.bfloat16)
        got = exchange(send, "tp", 1 << bit)
        now = [
            jnp.where(mine, b, a).astype(jnp.float32) + got[i].astype(jnp.float32)
            for i, (a, b) in enumerate(zip(low, high))
        ]
        bit += 1
        if (1 << bit) >= size:
            return now[0]
        low, high = now[0::2], now[1::2]


def body(
    query_wide,
    query_narrow,
    latent,
    rope_key,
    latent_norm_weight,
    broad_key_lift,
    broad_value_lift,
    slim_key_lift,
    slim_value_lift,
    out_wide,
    out_narrow,
    resid,
    ffn_gain,
    group_route,
    expert_pair,
    group_prob,
    expert_prob,
    gate_weight,
    up_weight,
    down_weight,
):
    tokens, rank = latent.shape
    groups = lax.axis_size("sp")
    tp_size = lax.axis_size("tp")
    place = lax.axis_index("sp")
    lane_place = lax.axis_index("tp")
    core = lane_place & 1
    half = tokens // 2
    capacity = 2 * tokens // groups
    model_width = resid.shape[1]
    quarter = model_width // tp_size
    f32, bf16 = jnp.float32, jnp.bfloat16

    share_of = group_prob[:, None] * expert_prob / jnp.sum(expert_prob, axis=1, keepdims=True)
    chosen = (expert_pair[:, :, None] == jnp.arange(EPG, dtype=jnp.int32)[None, None, :]).astype(f32)
    combine = jnp.sum(share_of[:, :, None] * chosen, axis=1)
    meta = jnp.concatenate(
        [
            combine,
            group_route.astype(f32)[:, None],
            jnp.zeros((tokens, LANES - ROPE - EPG - 1), f32),
        ],
        axis=1,
    )
    query_pos = place * tokens + jnp.arange(tokens, dtype=jnp.int32)
    angle_table = angles(query_pos, ROPE)
    cosine, sine = jnp.cos(angle_table), jnp.sin(angle_table)
    packed = call(pack_kernel, jax.ShapeDtypeStruct((tokens, rank + LANES), bf16), 6, smem=False)(
        latent, rope_key, latent_norm_weight[None, :], cosine, sine, meta
    )
    halves = packed.reshape(2, half, rank + LANES)
    own_half = jnp.where(core == 1, halves[1], halves[0])
    own_rest = jnp.where(core == 1, halves[0], halves[1])

    strides = list(range(2, groups, 2))
    got = {k: exchange(own_half, "sp", k) for k in reversed(strides)}
    column_got = [got[k] for k in strides]
    column = jnp.stack([own_half] + column_got)
    across = exchange(column, "sp", 1)
    column_rest = exchange(jnp.stack(column_got), "tp", 1)
    column_rest = jnp.concatenate([own_rest[None], column_rest], axis=0)
    across_rest = exchange(across, "tp", 1)

    heads_w = query_wide.shape[1] // (PLAIN_WIDTH_WIDE + ROPE)
    heads_n = query_narrow.shape[1] // (PLAIN_WIDTH_SLIM + ROPE)
    slim_lanes = heads_n * PLAIN_WIDTH_SLIM
    queries = []
    for source, heads, plain in (
        (query_wide, heads_w, PLAIN_WIDTH_WIDE),
        (query_narrow, heads_n, PLAIN_WIDTH_SLIM),
    ):
        for h in range(heads):
            part = source[:, h * (plain + ROPE) : (h + 1) * (plain + ROPE)]
            turned = turn(part[:, plain:].astype(f32), cosine, sine).astype(bf16)
            pieces = [part[:, :plain], turned, jnp.zeros((tokens, LANES - ROPE), bf16)]
            if plain == PLAIN_WIDTH_SLIM:
                before = jnp.zeros((tokens, h * plain), bf16)
                after = jnp.zeros((tokens, slim_lanes - (h + 1) * plain), bf16)
                pieces = [before, pieces[0], after] + pieces[1:]
            queries.append(jnp.concatenate(pieces, axis=1))
    queries = jnp.stack(queries)
    where = jnp.stack([place, core]).astype(jnp.int32)
    heads = heads_w + heads_n
    lifts = (broad_key_lift, broad_value_lift, slim_key_lift, slim_value_lift)
    state_shape = [jax.ShapeDtypeStruct((heads, tokens, LANES), f32)] * 3
    state = call(first_kernel, state_shape, 8, flops=10**9)(where, queries, column, column_rest, *lifts)
    piece_shape = jax.ShapeDtypeStruct((tp_size // 2, tokens, quarter), bf16)
    keep, send = call(second_kernel, [piece_shape] * 2, 13, flops=10**9)(
        where, queries, across, across_rest, *lifts, *state, out_wide, out_narrow
    )

    received = exchange(send, "tp", 1)
    paired = [keep[i].astype(f32) + received[i].astype(f32) for i in range(tp_size // 2)]
    summed = sum_scatter(paired[0::2], paired[1::2], 1, lane_place)
    resid_cols = lax.dynamic_slice_in_dim(resid, lane_place * quarter, quarter, 1)
    stream_cols = (resid_cols.astype(f32) + summed).astype(bf16)

    member = (group_route[:, None] == jnp.arange(groups, dtype=jnp.int32)[None, :]).astype(f32)
    upto = (jnp.arange(tokens)[:, None] >= jnp.arange(tokens)[None, :]).astype(f32)
    rank_of = jnp.sum(jnp.dot(upto, member) * member, axis=1).astype(jnp.int32) - 1
    slot_index = group_route * capacity + rank_of
    slot_hot = (slot_index[None, :] == jnp.arange(groups * capacity, dtype=jnp.int32)[:, None]).astype(bf16)

    first_part = jnp.concatenate([column[:, :, rank + ROPE : rank + ROPE + EPG + 1], across[:, :, rank + ROPE : rank + ROPE + EPG + 1]])
    second_part = jnp.concatenate([column_rest[:, :, rank + ROPE : rank + ROPE + EPG + 1], across_rest[:, :, rank + ROPE : rank + ROPE + EPG + 1]])
    gathered = jnp.where(
        core == 1,
        jnp.concatenate([second_part, first_part], axis=1),
        jnp.concatenate([first_part, second_part], axis=1),
    )
    here = (gathered[:, :, EPG].astype(jnp.int32) == place).astype(f32)
    order_here = jnp.einsum("kt,ut->ku", here, upto).astype(jnp.int32) - 1
    hot_here = (
        (order_here[:, None, :] == jnp.arange(capacity, dtype=jnp.int32)[None, :, None])
        & (here[:, None, :] > 0)
    ).astype(bf16)
    slot_weights = jnp.einsum("kct,kte->kce", hot_here, gathered[:, :, :EPG], preferred_element_type=f32)
    masks = jnp.arange(groups, dtype=jnp.int32)
    stack_of = jnp.where(masks & 1 == 1, groups // 2, 0) + (masks >> 1)
    pick = (stack_of[place ^ masks][:, None] == masks[None, :]).astype(f32)
    slot_weights = jnp.einsum("sk,kce->sce", pick, slot_weights, precision=lax.Precision.HIGHEST)
    slot_weights = slot_weights.reshape(groups * capacity, EPG)

    placed = dot(slot_hot, stream_cols).astype(bf16).reshape(groups, capacity, quarter)
    routed = lax.all_to_all(placed, "sp", split_axis=0, concat_axis=0, tiled=True)
    routed = routed.reshape(groups * capacity, quarter)
    parts = [routed]
    for bit in reversed(range(tp_size.bit_length() - 1)):
        parts = parts + [exchange(part, "tp", 1 << bit) for part in parts]
    masks_of = [0]
    for bit in reversed(range(tp_size.bit_length() - 1)):
        masks_of = masks_of + [m ^ (1 << bit) for m in masks_of]
    by_mask = [parts[masks_of.index(m)] for m in range(tp_size)]
    for bit in range(tp_size.bit_length() - 1):
        set_bit = ((lane_place >> bit) & 1) == 1
        by_mask = [jnp.where(set_bit, by_mask[m ^ (1 << bit)], by_mask[m]) for m in range(tp_size)]
    rows = jnp.concatenate(by_mask, axis=1).astype(f32)
    row_scale = lax.rsqrt(jnp.mean(rows * rows, axis=-1, keepdims=True) + EPSILON)
    normed = (rows * row_scale * ffn_gain).astype(bf16)
    gate_act = jnp.einsum("rd,edf->ref", normed, gate_weight[0], preferred_element_type=f32)
    up_act = jnp.einsum("rd,edf->ref", normed, up_weight[0], preferred_element_type=f32)
    hidden = (jax.nn.silu(gate_act) * up_act * slot_weights[:, :, None]).astype(bf16)
    partials = jnp.einsum("ref,efd->rd", hidden, down_weight[0], preferred_element_type=f32)
    cols = [partials[:, i * quarter : (i + 1) * quarter].astype(bf16) for i in range(tp_size)]
    summed_rows = sum_scatter(cols[0::2], cols[1::2], 0, lane_place).astype(bf16)
    returned = lax.all_to_all(
        summed_rows.reshape(groups, capacity, quarter), "sp", split_axis=0, concat_axis=0, tiled=True
    ).reshape(groups * capacity, quarter)
    moe_rows = lax.dot_general(slot_hot, returned, (((0,), (0,)), ((), ())), preferred_element_type=f32)
    return (stream_cols.astype(f32) + moe_rows).astype(bf16)


def solution(mesh):
    placed = (
        P("sp", "tp"),
        P("sp", "tp"),
        P("sp", None),
        P("sp", None),
        P(),
        P(None, "tp"),
        P(None, "tp"),
        P(None, "tp"),
        P(None, "tp"),
        P("tp", None),
        P("tp", None),
        P("sp", None),
        P(),
        P("sp"),
        P("sp", None),
        P("sp"),
        P("sp", None),
        P("sp", None, None, "tp"),
        P("sp", None, None, "tp"),
        P("sp", None, "tp", None),
    )
    return jax.shard_map(body, mesh=mesh, in_specs=placed, out_specs=P("sp", "tp"), check_vma=False)
```

```python
import functools

import jax
import jax.numpy as jnp
from jax import lax
from jax.experimental import pallas as pl
from jax.experimental.pallas import tpu as pltpu
from jax.sharding import PartitionSpec as P


PLAIN_WIDTH_WIDE = 128
PLAIN_WIDTH_SLIM = 64
ROPE = 64
VALUE_WIDTH_WIDE = 128
VALUE_WIDTH_SLIM = 64
EPG = 4
LANES = 128

ROPE_BASE = 10000.0
EPSILON = 1e-06
MASKED = -1e30


F32 = jnp.float32
BF16 = jnp.bfloat16
VMEM = pl.BlockSpec(memory_space=pltpu.VMEM)
HBM = pl.BlockSpec(memory_space=pltpu.HBM)


def angles(positions, width):
    frequency = 1.0 / ROPE_BASE ** (jnp.arange(0, width, 2).astype(F32) / width)
    return positions.astype(F32)[:, None] * frequency[None, :]


def turn(values, cosine, sine, axis):
    first_half, second = jnp.split(values, 2, axis=axis)
    return jnp.concatenate(
        [first_half * cosine - second * sine, second * cosine + first_half * sine], axis=axis
    )


def exchange(values, axis, mask):
    size = lax.axis_size(axis)
    return lax.ppermute(values, axis, [(i, i ^ mask) for i in range(size)])


def dot(a, b):
    return jnp.dot(a, b, preferred_element_type=F32)


def dot_t(a, b):
    return lax.dot_general(a, b, (((1,), (1,)), ((), ())), preferred_element_type=F32)


def iota(shape, dim):
    return lax.broadcasted_iota(jnp.int32, shape, dim)


def prefix_count(rows):
    size = rows.shape[1]
    upto = (iota((size, size), 0) <= iota((size, size), 1)).astype(BF16)
    return dot(rows.astype(BF16), upto)


def pack_kernel(
    cos_ref, sin_ref, latent_ref, rope_ref, gain_ref, route_ref, pair_ref, group_ref, prob_ref,
    half_ref, rest_ref,
):
    rank = latent_ref.shape[1]
    half = half_ref.shape[0]
    tokens = latent_ref.shape[0]
    odd = (lax.axis_index("tp") & 1) == 1
    widened = latent_ref[...].astype(F32)
    scale = lax.rsqrt(jnp.mean(widened * widened, axis=-1, keepdims=True) + EPSILON)
    normed = (widened * scale * gain_ref[...]).astype(BF16)
    turned = turn(rope_ref[...].astype(F32), cos_ref[...], sin_ref[...], 0)
    shares = group_ref[...] * prob_ref[...] / jnp.sum(prob_ref[...], axis=0, keepdims=True)
    rows = iota((LANES - ROPE, tokens), 0)
    meta = jnp.where(rows == EPG, route_ref[...].astype(F32), 0.0)
    for expert in range(EPG):
        chosen = jnp.sum(jnp.where(pair_ref[...] == expert, shares, 0.0), axis=0, keepdims=True)
        meta = jnp.where(rows == expert, chosen, meta)
    tail = jnp.concatenate([turned, meta], axis=0).T.astype(BF16)
    half_ref[:, :rank] = jnp.where(odd, normed[half:], normed[:half])
    half_ref[:, rank:] = jnp.where(odd, tail[half:], tail[:half])
    rest_ref[:, :rank] = jnp.where(odd, normed[:half], normed[half:])
    rest_ref[:, rank:] = jnp.where(odd, tail[:half], tail[half:])


def query_kernel(cos_ref, sin_ref, wide_ref, slim_ref, out_ref):
    tokens = wide_ref.shape[0]
    heads_w = wide_ref.shape[1] // (PLAIN_WIDTH_WIDE + ROPE)
    heads_n = slim_ref.shape[1] // (PLAIN_WIDTH_SLIM + ROPE)
    cosine, sine = cos_ref[...], sin_ref[...]
    spare = jnp.zeros((tokens, LANES - ROPE), F32)
    for h in range(heads_w + heads_n):
        wide = h < heads_w
        plain = PLAIN_WIDTH_WIDE if wide else PLAIN_WIDTH_SLIM
        start = (h if wide else h - heads_w) * (plain + ROPE)
        part = (wide_ref if wide else slim_ref)[:, start : start + plain + ROPE].astype(F32)
        pieces = [part[:, :plain], turn(part[:, plain:], cosine, sine, 1), spare]
        if not wide:
            before = (h - heads_w) * plain
            after = heads_n * plain - before - plain
            if before:
                pieces = [jnp.zeros((tokens, before), F32)] + pieces
            if after:
                pieces = pieces[:-2] + [jnp.zeros((tokens, after), F32)] + pieces[-2:]
        out_ref[h] = jnp.concatenate(pieces, axis=1).astype(BF16)


def pieces_of(refs):
    return [
        piece
        for ref in refs
        for piece in ([ref[...]] if len(ref.shape) == 2 else [ref[i] for i in range(ref.shape[0])])
    ]


def attend_body(q_ref, stacks, kw_ref, vw_ref, kn_ref, vn_ref, state, masks):
    count = len(stacks) // 2
    mine, other = pieces_of(stacks[:count]), pieces_of(stacks[count:])
    heads_w = kw_ref.shape[1] // PLAIN_WIDTH_WIDE
    heads_n = kn_ref.shape[1] // PLAIN_WIDTH_SLIM
    half = mine[0].shape[0]
    tokens = q_ref.shape[1]
    rank = kw_ref.shape[0]
    place = lax.axis_index("sp")
    core = lax.axis_index("tp") & 1
    shift = half.bit_length() - 1
    step = 5
    for start in range(0, len(mine), step):
        group = mine[start : start + step]
        rows = len(group) * half
        lat = jnp.concatenate(group + other[start : start + step], axis=0)
        flat = lat[:, :rank]
        rot = lat[:, rank:]
        key_w = dot(flat, kw_ref[...]).astype(BF16)
        key_n = dot(flat, kn_ref[...]).astype(BF16)
        val_w = dot(flat, vw_ref[...]).astype(BF16)
        val_n = dot(flat, vn_ref[...]).astype(BF16)
        lane = iota((1, 2 * rows), 1)
        first = lane < rows
        inner = jnp.where(first, lane, lane - rows)
        piece = inner >> shift
        mask = jnp.zeros_like(piece)
        for i in range(len(group)):
            mask = jnp.where(piece == i, masks[start + i], mask)
        block = place ^ mask
        offset = jnp.where(first, core, 1 - core)
        key_pos = (block * 2 + offset) * half + (inner & (half - 1))
        visible = iota((tokens, 1), 0) + place * tokens >= key_pos
        new_state = []
        for h in range(heads_w + heads_n):
            if h < heads_w:
                keys = key_w[:, h * PLAIN_WIDTH_WIDE : (h + 1) * PLAIN_WIDTH_WIDE]
                values = val_w[:, h * VALUE_WIDTH_WIDE : (h + 1) * VALUE_WIDTH_WIDE]
                scale = (PLAIN_WIDTH_WIDE + ROPE) ** (-0.5)
            else:
                keys = key_n
                values = val_n
                scale = (PLAIN_WIDTH_SLIM + ROPE) ** (-0.5)
            scores = dot_t(q_ref[h], jnp.concatenate([keys, rot], axis=1)) * scale
            scores = jnp.where(visible, scores, MASKED)
            peak = jnp.max(scores, axis=-1, keepdims=True)
            if state is not None:
                peak = jnp.maximum(peak, state[h][0])
            weights = jnp.exp(scores - peak)
            total = jnp.sum(weights, axis=-1, keepdims=True)
            acc = dot(weights.astype(BF16), values)
            if state is not None:
                keep = jnp.exp(state[h][0] - peak)
                total = total + state[h][1] * keep
                acc = acc + state[h][2] * keep
            new_state.append((peak, total, acc))
        state = new_state
    return state


def first_kernel(masks, *refs):
    q_ref, kw_ref, vw_ref, kn_ref, vn_ref = refs[:5]
    peak_ref, total_ref, acc_ref = refs[-3:]
    state = attend_body(q_ref, refs[5:-3], kw_ref, vw_ref, kn_ref, vn_ref, None, masks)
    for h, (peak, total, acc) in enumerate(state):
        peak_ref[h] = jnp.broadcast_to(peak, peak_ref.shape[1:])
        total_ref[h] = jnp.broadcast_to(total, total_ref.shape[1:])
        acc_ref[h] = acc


def second_kernel(masks, *refs):
    q_ref, kw_ref, vw_ref, kn_ref, vn_ref, peak_ref, total_ref, acc_ref, ow_ref, on_ref = refs[:10]
    keep_ref, send_ref = refs[-2:]
    heads = peak_ref.shape[0]
    heads_w = kw_ref.shape[1] // PLAIN_WIDTH_WIDE
    state = [(peak_ref[h, :, :1], total_ref[h, :, :1], acc_ref[h]) for h in range(heads)]
    state = attend_body(q_ref, refs[10:-2], kw_ref, vw_ref, kn_ref, vn_ref, state, masks)
    done = [acc / total for _, total, acc in state]
    att_w = jnp.concatenate(done[:heads_w], axis=1).astype(BF16)
    slim = done[heads_w]
    for h in range(1, heads - heads_w):
        lane = iota(slim.shape, 1)
        slim = jnp.where(lane >= h * VALUE_WIDTH_SLIM, done[heads_w + h], slim)
    att_n = slim.astype(BF16)
    core = lax.axis_index("tp") & 1
    project(att_w, att_n, ow_ref, on_ref, send_ref, 1 - core)
    project(att_w, att_n, ow_ref, on_ref, keep_ref, core)


def project(att_w, att_n, ow_ref, on_ref, out_ref, bit):
    pieces, _, quarter = out_ref.shape
    for piece in range(pieces):
        cols = pl.ds(pl.multiple_of((2 * piece + bit) * quarter, LANES), quarter)
        out_ref[piece] = (dot(att_w, ow_ref[:, cols]) + dot(att_n, on_ref[:, cols])).astype(BF16)


def slots_of(route, groups, capacity):
    tokens = route.shape[1]
    member = (iota((groups, tokens), 0) == route).astype(F32)
    rank_of = jnp.sum(prefix_count(member) * member, axis=0, keepdims=True).astype(jnp.int32) - 1
    slot = route * capacity + rank_of
    return (iota((groups * capacity, tokens), 0) == slot).astype(BF16)


def weights_kernel(masks, *refs):
    out_ref = refs[-1]
    count = (len(refs) - 1) // 2
    mine_all, other_all = pieces_of(refs[:count]), pieces_of(refs[count:-1])
    half, width = mine_all[0].shape
    place = lax.axis_index("sp")
    odd = (lax.axis_index("tp") & 1) == 1
    capacity = out_ref.shape[0] // len(mine_all)
    base = width - LANES
    for mask, mine, other in zip(masks, mine_all, other_all):
        mine, other = mine[:, base:], other[:, base:]
        data = jnp.concatenate(
            [jnp.where(odd, other, mine), jnp.where(odd, mine, other)], axis=0
        )
        route = data.astype(F32).T[ROPE + EPG : ROPE + EPG + 1]
        here = (route == place.astype(F32)).astype(F32)
        order = prefix_count(here) - 1.0
        hot = jnp.where((iota((capacity, 2 * half), 0).astype(F32) == order) & (here > 0), 1.0, 0.0)
        start = pl.multiple_of((place ^ mask) * capacity, capacity)
        out_ref[pl.ds(start, capacity), :] = dot(hot.astype(BF16), data)


def place_kernel(keep_ref, got_ref, resid_ref, route_ref, stream_ref, placed_ref):
    groups, capacity, _ = placed_ref.shape
    stream = keep_ref[...].astype(F32) + got_ref[...].astype(F32) + resid_ref[...].astype(F32)
    stream = stream.astype(BF16)
    stream_ref[...] = stream
    hot = slots_of(route_ref[...], groups, capacity)
    placed_ref[...] = dot(hot, stream).astype(BF16).reshape(placed_ref.shape)


def final_kernel(stream_ref, back_ref, route_ref, out_ref):
    groups, copies, capacity, quarter = back_ref.shape
    hot = slots_of(route_ref[...], groups, capacity)
    total = stream_ref[...].astype(F32)
    for copy in range(copies):
        rows = back_ref[:, copy].reshape(groups * capacity, quarter)
        total = total + lax.dot_general(hot, rows, (((0,), (0,)), ((), ())), preferred_element_type=F32)
    out_ref[...] = total.astype(BF16)


def expand_part(masks, gain_ref, gate_ref, up_ref, parts, acts, square):
    quarter = parts[0].shape[1]
    place = lax.axis_index("tp")
    for mask, part in zip(masks, parts):
        cols = pl.ds(pl.multiple_of((place ^ mask) * quarter, LANES), quarter)
        rows = part[...].astype(F32)
        square = square + jnp.sum(rows * rows, axis=-1, keepdims=True)
        scaled = (rows * gain_ref[:, cols]).astype(BF16)
        for e in range(len(acts)):
            both = jnp.concatenate([gate_ref[e, cols, :], up_ref[e, cols, :]], axis=1)
            acts[e] = acts[e] + dot(scaled, both)
    return square


def near_kernel(masks, gain_ref, gate_ref, up_ref, *refs):
    act_ref, square_ref = refs[-2:]
    acts = [0.0] * act_ref.shape[0]
    square = expand_part(masks, gain_ref, gate_ref, up_ref, refs[:-2], acts, 0.0)
    for e, act in enumerate(acts):
        act_ref[e] = act
    square_ref[...] = jnp.broadcast_to(square, square_ref.shape)


def contract(hidden, down_ref, out_ref, bit):
    groups, uppers, capacity, quarter = out_ref.shape
    for upper in range(uppers):
        cols = pl.ds(pl.multiple_of((2 * upper + bit) * quarter, LANES), quarter)
        out_ref[:, upper] = dot(hidden, down_ref[:, cols]).astype(BF16).reshape(groups, capacity, quarter)


def far_kernel(masks, gain_ref, gate_ref, up_ref, down_ref, weight_ref, act_ref, square_ref, *refs):
    send_ref, hidden_ref = refs[-2:]
    experts, model_width, hidden_width = gate_ref.shape
    acts = [act_ref[e] for e in range(experts)]
    square = expand_part(masks, gain_ref, gate_ref, up_ref, refs[:-2], acts, square_ref[:, :1])
    scale = lax.rsqrt(square / model_width + EPSILON)
    hidden = []
    for e in range(experts):
        gate, up = acts[e][:, :hidden_width] * scale, acts[e][:, hidden_width:] * scale
        weight = weight_ref[:, ROPE + e : ROPE + e + 1]
        hidden.append((gate / (1.0 + jnp.exp(-gate)) * up * weight).astype(BF16))
    hidden = jnp.concatenate(hidden, axis=1)
    hidden_ref[...] = hidden
    contract(hidden, down_ref, send_ref, 1 - (lax.axis_index("tp") & 1))


def stay_kernel(hidden_ref, down_ref, keep_ref):
    contract(hidden_ref[...], down_ref, keep_ref, lax.axis_index("tp") & 1)


def start_copies(sources, targets, semaphores):
    copies = [
        pltpu.make_async_copy(source, target, semaphores.at[i])
        for i, (source, target) in enumerate(zip(sources, targets))
    ]
    for copy in copies:
        copy.start()
    return copies


def call(kernel, outs, inputs, fetched=(), kept=(), mib=12):
    n_in, n_fetched, n_kept, n_out = len(inputs), len(fetched), len(kept), len(outs)

    def wrapped(*refs):
        refs = list(refs)
        take = lambda n: [refs.pop(0) for _ in range(n)]
        ins, sources, kept_sources = take(n_in), take(n_fetched), take(n_kept)
        results, kept_results, held = take(n_out), take(n_kept), take(n_fetched)
        first = start_copies(sources, held, refs[0]) if n_fetched else []
        second = start_copies(kept_sources, kept_results, refs[-1]) if n_kept else []
        for copy in first:
            copy.wait()
        kernel(*ins, *held, *results)
        for copy in second:
            copy.wait()

    semaphores = [pltpu.SemaphoreType.DMA((n,)) for n in (n_fetched, n_kept) if n]
    return pl.pallas_call(
        wrapped,
        out_shape=list(outs) + [held_shape(a.shape, a.dtype) for a in kept],
        in_specs=[VMEM] * n_in + [HBM] * (n_fetched + n_kept),
        out_specs=[VMEM] * (n_out + n_kept),
        scratch_shapes=[pltpu.VMEM(a.shape, a.dtype) for a in fetched] + semaphores,
        compiler_params=pltpu.CompilerParams(vmem_limit_bytes=mib * 2**20),
    )(
        *(pltpu.with_memory_space_constraint(a, pltpu.VMEM) for a in inputs),
        *(pltpu.with_memory_space_constraint(a, pltpu.HBM) for a in (*fetched, *kept)),
    )


def shape(dims, dtype=BF16):
    return jax.ShapeDtypeStruct(dims, dtype)


def held_shape(dims, dtype=BF16):
    return pltpu.VMEM(dims, dtype)


def halved(keep, got, first_bit, place):
    pieces = [keep[i].astype(F32) + got[i].astype(F32) for i in range(keep.shape[0])]
    bit = first_bit
    while True:
        mine = ((place >> bit) & 1) == 1
        low, high = pieces[0::2], pieces[1::2]
        send = [jnp.where(mine, a, b).astype(BF16) for a, b in zip(low, high)]
        stay = [jnp.where(mine, b, a) for a, b in zip(low, high)]
        if len(send) == 1:
            return stay[0].astype(BF16), exchange(send[0], "tp", 1 << bit)
        came = exchange(jnp.stack(send), "tp", 1 << bit)
        pieces = [a + came[i].astype(F32) for i, a in enumerate(stay)]
        bit += 1


def body(
    query_wide,
    query_narrow,
    latent,
    rope_key,
    latent_norm_weight,
    broad_key_lift,
    broad_value_lift,
    slim_key_lift,
    slim_value_lift,
    out_wide,
    out_narrow,
    resid,
    ffn_gain,
    group_route,
    expert_pair,
    group_prob,
    expert_prob,
    gate_weight,
    up_weight,
    down_weight,
):
    tokens, rank = latent.shape
    groups = lax.axis_size("sp")
    tp_size = lax.axis_size("tp")
    place = lax.axis_index("sp")
    lane_place = lax.axis_index("tp")
    half = tokens // 2
    capacity = 2 * tokens // groups
    slots = groups * capacity
    model_width = resid.shape[1]
    quarter = model_width // tp_size
    route = group_route[None, :]

    query_pos = place * tokens + jnp.arange(tokens, dtype=jnp.int32)
    table = angles(query_pos, ROPE).T
    packed = held_shape((half, rank + LANES))
    own, rest = call(
        pack_kernel, [packed, packed], [jnp.cos(table), jnp.sin(table)],
        [latent, rope_key.T, latent_norm_weight[None, :], route, expert_pair.T, group_prob[None, :], expert_prob.T],
        mib=4,
    )

    strides = list(range(groups - 2, 0, -2))
    got = []
    for k in strides:
        got.append(exchange(own, "sp", k))
    across = [exchange(own, "sp", 1)]
    across_rest = [exchange(across[0], "tp", 1)]
    cut = len(strides) // 2
    for pieces in (got[:cut], got[cut:]):
        across.append(exchange(jnp.stack(pieces), "sp", 1))
    column = [own, jnp.stack(got)]
    column_rest = [rest, exchange(column[1], "tp", 1)]
    across = [across[0], jnp.concatenate(across[1:])]
    across_rest.append(exchange(across[1], "tp", 1))
    first_masks = [0] + strides + [1]
    second_masks = [k ^ 1 for k in strides]

    heads = query_wide.shape[1] // (PLAIN_WIDTH_WIDE + ROPE) + query_narrow.shape[1] // (PLAIN_WIDTH_SLIM + ROPE)
    angle_rows = angles(query_pos, ROPE)
    queries, key_w, value_w, key_n, value_n, out_w, out_n = call(
        query_kernel, [held_shape((heads, tokens, 2 * LANES))], [jnp.cos(angle_rows), jnp.sin(angle_rows)],
        [query_wide, query_narrow],
        [broad_key_lift, broad_value_lift, slim_key_lift, slim_value_lift, out_wide, out_narrow], mib=4,
    )
    lifts = [key_w, value_w, key_n, value_n]
    state = call(
        functools.partial(first_kernel, first_masks), [held_shape((heads, tokens, LANES), F32)] * 3,
        [queries, *lifts, *column, across[0], *column_rest, across_rest[0]],
    )
    pieces_shape = held_shape((tp_size // 2, tokens, quarter))
    keep, send = call(
        functools.partial(second_kernel, second_masks), [pieces_shape] * 2,
        [queries, *lifts, *state, out_w, out_n, *across[1:], *across_rest[1:]],
    )
    slot_weights, gate, up, down, gain = call(
        functools.partial(weights_kernel, first_masks + second_masks), [held_shape((slots, LANES), F32)],
        [*column, *across, *column_rest, *across_rest], [],
        [gate_weight[0], up_weight[0], down_weight[0].reshape(-1, model_width), ffn_gain[None, :]], mib=4,
    )

    received = exchange(send, "tp", 1)
    stay, came = halved(keep, received, 1, lane_place)
    resid_cols = lax.dynamic_slice_in_dim(resid, lane_place * quarter, quarter, 1)
    stream_cols, placed = call(
        place_kernel, [held_shape((tokens, quarter)), held_shape((groups, capacity, quarter))],
        [stay, came, resid_cols, route], mib=4,
    )

    routed = lax.all_to_all(placed, "sp", split_axis=0, concat_axis=0, tiled=True)
    routed = routed.reshape(slots, quarter)
    far_masks = list(range(2, tp_size, 2))
    far = []
    for mask in far_masks:
        far.append(exchange(routed, "tp", mask))
    near = exchange(routed, "tp", 1)
    experts, _, hidden_width = gate_weight[0].shape
    acts, square = call(
        functools.partial(near_kernel, [0, 1]),
        [held_shape((experts, slots, 2 * hidden_width), F32), held_shape((slots, LANES), F32)],
        [gain, gate, up, routed, near],
    )
    far_near = [exchange(part, "tp", 1) for part in far]
    uppers = tp_size // 2
    cube = held_shape((groups, uppers, capacity, quarter))
    send, hidden = call(
        functools.partial(far_kernel, far_masks + [m | 1 for m in far_masks]),
        [cube, held_shape((slots, experts * hidden_width))],
        [gain, gate, up, down, slot_weights, acts, square, *far, *far_near],
    )
    received = exchange(send, "tp", 1)
    (keep,) = call(stay_kernel, [cube], [hidden, down])

    teams = [
        [g * tp_size + 2 * upper + low for g in range(groups) for upper in range(uppers)] for low in range(2)
    ]
    summed = (keep.astype(F32) + received.astype(F32)).astype(BF16)
    returned = lax.all_to_all(
        summed.reshape(groups * uppers, capacity, quarter),
        ("sp", "tp"), split_axis=0, concat_axis=0, axis_index_groups=teams, tiled=True,
    ).reshape(cube.shape)
    return call(final_kernel, [shape((tokens, quarter))], [stream_cols, returned, route], mib=4)[0]


def solution(mesh):
    placed = (
        P("sp", "tp"),
        P("sp", "tp"),
        P("sp", None),
        P("sp", None),
        P(),
        P(None, "tp"),
        P(None, "tp"),
        P(None, "tp"),
        P(None, "tp"),
        P("tp", None),
        P("tp", None),
        P("sp", None),
        P(),
        P("sp"),
        P("sp", None),
        P("sp"),
        P("sp", None),
        P("sp", None, None, "tp"),
        P("sp", None, None, "tp"),
        P("sp", None, "tp", None),
    )
    return jax.shard_map(body, mesh=mesh, in_specs=placed, out_specs=P("sp", "tp"), check_vma=False)
```

```python
import functools

import jax
import jax.numpy as jnp
from jax import lax
from jax.experimental import pallas as pl
from jax.experimental.pallas import tpu as pltpu
from jax.sharding import PartitionSpec as P


PLAIN_WIDTH_WIDE = 128
PLAIN_WIDTH_SLIM = 64
ROPE = 64
VALUE_WIDTH_WIDE = 128
VALUE_WIDTH_SLIM = 64
EPG = 4
LANES = 128

ROPE_BASE = 10000.0
EPSILON = 1e-06
MASKED = -1e30


F32 = jnp.float32
BF16 = jnp.bfloat16
VMEM = pl.BlockSpec(memory_space=pltpu.VMEM)
HBM = pl.BlockSpec(memory_space=pltpu.HBM)


def angles(positions, width):
    frequency = 1.0 / ROPE_BASE ** (jnp.arange(0, width, 2).astype(F32) / width)
    return positions.astype(F32)[:, None] * frequency[None, :]


def turn(values, cosine, sine, axis):
    first_half, second = jnp.split(values, 2, axis=axis)
    return jnp.concatenate(
        [first_half * cosine - second * sine, second * cosine + first_half * sine], axis=axis
    )


def exchange(values, axis, mask):
    size = lax.axis_size(axis)
    return lax.ppermute(values, axis, [(i, i ^ mask) for i in range(size)])


def dot(a, b):
    return jnp.dot(a, b, preferred_element_type=F32)


def dot_t(a, b):
    return lax.dot_general(a, b, (((1,), (1,)), ((), ())), preferred_element_type=F32)


def iota(shape, dim):
    return lax.broadcasted_iota(jnp.int32, shape, dim)


def prefix_count(rows):
    size = rows.shape[1]
    upto = (iota((size, size), 0) <= iota((size, size), 1)).astype(BF16)
    return dot(rows.astype(BF16), upto)


def pack_kernel(
    cos_ref, sin_ref, latent_ref, rope_ref, gain_ref, route_ref, pair_ref, group_ref, prob_ref,
    half_ref, rest_ref,
):
    rank = latent_ref.shape[1]
    half = half_ref.shape[0]
    tokens = latent_ref.shape[0]
    odd = (lax.axis_index("tp") & 1) == 1
    widened = latent_ref[...].astype(F32)
    scale = lax.rsqrt(jnp.mean(widened * widened, axis=-1, keepdims=True) + EPSILON)
    normed = (widened * scale * gain_ref[...]).astype(BF16)
    turned = turn(rope_ref[...].astype(F32), cos_ref[...], sin_ref[...], 0)
    shares = group_ref[...] * prob_ref[...] / jnp.sum(prob_ref[...], axis=0, keepdims=True)
    rows = iota((LANES - ROPE, tokens), 0)
    meta = jnp.where(rows == EPG, route_ref[...].astype(F32), 0.0)
    for expert in range(EPG):
        chosen = jnp.sum(jnp.where(pair_ref[...] == expert, shares, 0.0), axis=0, keepdims=True)
        meta = jnp.where(rows == expert, chosen, meta)
    tail = jnp.concatenate([turned, meta], axis=0).T.astype(BF16)
    half_ref[:, :rank] = jnp.where(odd, normed[half:], normed[:half])
    half_ref[:, rank:] = jnp.where(odd, tail[half:], tail[:half])
    rest_ref[:, :rank] = jnp.where(odd, normed[:half], normed[half:])
    rest_ref[:, rank:] = jnp.where(odd, tail[:half], tail[half:])


def query_kernel(cos_ref, sin_ref, wide_ref, slim_ref, out_ref):
    tokens = wide_ref.shape[0]
    heads_w = wide_ref.shape[1] // (PLAIN_WIDTH_WIDE + ROPE)
    heads_n = slim_ref.shape[1] // (PLAIN_WIDTH_SLIM + ROPE)
    spare = jnp.zeros((tokens, LANES - ROPE), F32)
    cosine, sine = cos_ref[...].T, sin_ref[...].T
    for h in range(heads_w + heads_n):
        wide = h < heads_w
        plain = PLAIN_WIDTH_WIDE if wide else PLAIN_WIDTH_SLIM
        start = (h if wide else h - heads_w) * (plain + ROPE)
        part = (wide_ref if wide else slim_ref)[:, start : start + plain + ROPE].astype(F32)
        pieces = [part[:, :plain], turn(part[:, plain:], cosine, sine, 1), spare]
        if not wide:
            before = (h - heads_w) * plain
            after = heads_n * plain - before - plain
            if before:
                pieces = [jnp.zeros((tokens, before), F32)] + pieces
            if after:
                pieces = pieces[:-2] + [jnp.zeros((tokens, after), F32)] + pieces[-2:]
        out_ref[h] = jnp.concatenate(pieces, axis=1).astype(BF16)


def pieces_of(refs):
    return [
        piece
        for ref in refs
        for piece in ([ref[...]] if len(ref.shape) == 2 else [ref[i] for i in range(ref.shape[0])])
    ]


def attend_body(queries, pieces, masks, mine, kw_ref, vw_ref, kn_ref, vn_ref, state):
    heads_w = kw_ref.shape[1] // PLAIN_WIDTH_WIDE
    heads_n = kn_ref.shape[1] // PLAIN_WIDTH_SLIM
    half = pieces[0].shape[0]
    tokens = queries[0].shape[0]
    rank = kw_ref.shape[0]
    place = lax.axis_index("sp")
    core = lax.axis_index("tp") & 1
    shift = half.bit_length() - 1
    step = 8
    for start in range(0, len(pieces), step):
        group = pieces[start : start + step]
        rows = len(group) * half
        lat = jnp.concatenate(group, axis=0)
        flat = lat[:, :rank]
        rot = lat[:, rank:]
        key_w = dot(flat, kw_ref[...]).astype(BF16)
        key_n = dot(flat, kn_ref[...]).astype(BF16)
        val_w = dot(flat, vw_ref[...]).astype(BF16)
        val_n = dot(flat, vn_ref[...]).astype(BF16)
        lane = iota((1, rows), 1)
        index = lane >> shift
        mask = jnp.zeros_like(lane)
        offset = jnp.zeros_like(lane)
        for i in range(len(group)):
            mask = jnp.where(index == i, masks[start + i], mask)
            offset = jnp.where(index == i, core if mine[start + i] else 1 - core, offset)
        key_pos = ((place ^ mask) * 2 + offset) * half + (lane & (half - 1))
        visible = iota((tokens, 1), 0) + place * tokens >= key_pos
        new_state = []
        for h in range(heads_w + heads_n):
            if h < heads_w:
                keys = key_w[:, h * PLAIN_WIDTH_WIDE : (h + 1) * PLAIN_WIDTH_WIDE]
                values = val_w[:, h * VALUE_WIDTH_WIDE : (h + 1) * VALUE_WIDTH_WIDE]
                scale = (PLAIN_WIDTH_WIDE + ROPE) ** (-0.5)
            else:
                keys = key_n
                values = val_n
                scale = (PLAIN_WIDTH_SLIM + ROPE) ** (-0.5)
            scores = dot_t(queries[h], jnp.concatenate([keys, rot], axis=1)) * scale
            scores = jnp.where(visible, scores, MASKED)
            peak = jnp.max(scores, axis=-1, keepdims=True)
            if state is not None:
                peak = jnp.maximum(peak, state[h][0])
            weights = jnp.exp(scores - peak)
            total = jnp.sum(weights, axis=-1, keepdims=True)
            acc = dot(weights.astype(BF16), values)
            if state is not None:
                keep = jnp.exp(state[h][0] - peak)
                total = total + state[h][1] * keep
                acc = acc + state[h][2] * keep
            new_state.append((peak, total, acc))
        state = new_state
    return state


def store_state(state, refs):
    peak_ref, total_ref, acc_ref = refs
    for h, (peak, total, acc) in enumerate(state):
        peak_ref[h] = jnp.broadcast_to(peak, peak_ref.shape[1:])
        total_ref[h] = jnp.broadcast_to(total, total_ref.shape[1:])
        acc_ref[h] = acc


def load_state(refs):
    peak_ref, total_ref, acc_ref = refs
    return [(peak_ref[h, :, :1], total_ref[h, :, :1], acc_ref[h]) for h in range(peak_ref.shape[0])]


def first_kernel(masks, q_ref, *refs):
    lifts, blocks = refs[:4], refs[4:-3]
    queries = [q_ref[h] for h in range(q_ref.shape[0])]
    mine = [True] * len(masks) + [False] * len(masks)
    store_state(attend_body(queries, pieces_of(blocks), masks * 2, mine, *lifts, None), refs[-3:])


def second_kernel(masks, q_ref, *refs):
    lifts, state_refs, blocks = refs[:4], refs[4:7], refs[7:-3]
    queries = [q_ref[h] for h in range(q_ref.shape[0])]
    state = attend_body(queries, pieces_of(blocks), masks, [True] * len(masks), *lifts, load_state(state_refs))
    store_state(state, refs[-3:])


def third_kernel(masks, q_ref, *refs):
    lifts, state_refs, (ow_ref, on_ref), blocks = refs[:4], refs[4:7], refs[7:9], refs[9:-2]
    keep_ref, send_ref = refs[-2:]
    queries = [q_ref[h] for h in range(q_ref.shape[0])]
    heads = len(queries)
    heads_w = lifts[0].shape[1] // PLAIN_WIDTH_WIDE
    state = attend_body(queries, pieces_of(blocks), masks, [False] * len(masks), *lifts, load_state(state_refs))
    done = [acc / total for _, total, acc in state]
    att_w = jnp.concatenate(done[:heads_w], axis=1).astype(BF16)
    slim = done[heads_w]
    for h in range(1, heads - heads_w):
        lane = iota(slim.shape, 1)
        slim = jnp.where(lane >= h * VALUE_WIDTH_SLIM, done[heads_w + h], slim)
    att_n = slim.astype(BF16)
    core = lax.axis_index("tp") & 1
    project(att_w, att_n, ow_ref, on_ref, send_ref, 1 - core)
    project(att_w, att_n, ow_ref, on_ref, keep_ref, core)


def project(att_w, att_n, ow_ref, on_ref, out_ref, bit):
    pieces, _, quarter = out_ref.shape
    for piece in range(pieces):
        cols = pl.ds(pl.multiple_of((2 * piece + bit) * quarter, LANES), quarter)
        out_ref[piece] = (dot(att_w, ow_ref[:, cols]) + dot(att_n, on_ref[:, cols])).astype(BF16)


def slots_of(route, groups, capacity):
    tokens = route.shape[1]
    member = (iota((groups, tokens), 0) == route).astype(F32)
    rank_of = jnp.sum(prefix_count(member) * member, axis=0, keepdims=True).astype(jnp.int32) - 1
    slot = route * capacity + rank_of
    return (iota((groups * capacity, tokens), 0) == slot).astype(BF16)


def weights_kernel(masks, route_ref, *refs):
    refs, hot_ref = refs[:-1], refs[-1]
    out_ref = refs[-1]
    count = (len(refs) - 1) // 2
    mine_all, other_all = pieces_of(refs[:count]), pieces_of(refs[count:-1])
    half, width = mine_all[0].shape
    place = lax.axis_index("sp")
    odd = (lax.axis_index("tp") & 1) == 1
    capacity = out_ref.shape[0] // len(mine_all)
    base = width - LANES
    hot_ref[...] = slots_of(route_ref[...], len(mine_all), capacity)
    for mask, mine, other in zip(masks, mine_all, other_all):
        mine, other = mine[:, base:], other[:, base:]
        data = jnp.concatenate(
            [jnp.where(odd, other, mine), jnp.where(odd, mine, other)], axis=0
        )
        route = data.astype(F32).T[ROPE + EPG : ROPE + EPG + 1]
        here = (route == place.astype(F32)).astype(F32)
        order = prefix_count(here) - 1.0
        hot = jnp.where((iota((capacity, 2 * half), 0).astype(F32) == order) & (here > 0), 1.0, 0.0)
        start = pl.multiple_of((place ^ mask) * capacity, capacity)
        out_ref[pl.ds(start, capacity), :] = dot(hot.astype(BF16), data)


def pair_kernel(masks, keep_ref, got_ref, stay_ref, *send_refs):
    upper = lax.axis_index("tp") >> 1
    for ref, mask in zip((stay_ref, *send_refs), [0] + masks):
        piece = upper ^ (mask >> 1)
        ref[...] = (keep_ref[piece].astype(F32) + got_ref[piece].astype(F32)).astype(BF16)


def place_kernel(resid_ref, hot_ref, *refs):
    stream_ref, placed_ref = refs[-2:]
    stream = resid_ref[...].astype(F32)
    for ref in refs[:-2]:
        stream = stream + ref[...].astype(F32)
    stream = stream.astype(BF16)
    stream_ref[...] = stream
    placed_ref[...] = dot(hot_ref[...], stream).astype(BF16).reshape(placed_ref.shape)


def final_kernel(stream_ref, back_ref, hot_ref, out_ref):
    groups, capacity, quarter = back_ref.shape
    rows = back_ref[...].reshape(groups * capacity, quarter)
    moe = lax.dot_general(hot_ref[...], rows, (((0,), (0,)), ((), ())), preferred_element_type=F32)
    out_ref[...] = (stream_ref[...].astype(F32) + moe).astype(BF16)


def expand_part(masks, gain_ref, gate_ref, up_ref, parts, acts, square):
    quarter = parts[0].shape[1]
    place = lax.axis_index("tp")
    for mask, part in zip(masks, parts):
        cols = pl.ds(pl.multiple_of((place ^ mask) * quarter, LANES), quarter)
        rows = part[...].astype(F32)
        square = square + jnp.sum(rows * rows, axis=-1, keepdims=True)
        scaled = (rows * gain_ref[:, cols]).astype(BF16)
        for e in range(len(acts)):
            both = jnp.concatenate([gate_ref[e, cols, :], up_ref[e, cols, :]], axis=1)
            acts[e] = acts[e] + dot(scaled, both)
    return square


def near_kernel(masks, gain_ref, gate_ref, up_ref, *refs):
    act_ref, square_ref = refs[-2:]
    acts = [0.0] * act_ref.shape[0]
    square = expand_part(masks, gain_ref, gate_ref, up_ref, refs[:-2], acts, 0.0)
    for e, act in enumerate(acts):
        act_ref[e] = act
    square_ref[...] = jnp.broadcast_to(square, square_ref.shape)


def places_of(weight_ref, span, experts):
    firsts, seconds = [], []
    seen = 0.0
    for e in range(experts):
        chosen = jnp.where(weight_ref[span, ROPE + e : ROPE + e + 1] != 0.0, 1.0, 0.0)
        firsts.append((chosen > 0.0) & (seen == 0.0))
        seconds.append((chosen > 0.0) & (seen == 1.0))
        seen = seen + chosen
    return firsts, seconds


def far_kernel(masks, gain_ref, gate_ref, up_ref, weight_ref, act_ref, square_ref, *refs):
    hidden_ref, pair_ref = refs[-2:]
    halves = (refs[: len(masks)], refs[len(masks) : -2])
    experts, model_width, hidden_width = gate_ref.shape
    rows = hidden_ref.shape[0] // 2
    for first, parts in zip((0, rows), halves):
        span = slice(first, first + rows)
        acts = [act_ref[e, span, :] for e in range(experts)]
        square = expand_part(masks, gain_ref, gate_ref, up_ref, parts, acts, square_ref[span, :1])
        scale = lax.rsqrt(square / model_width + EPSILON)
        firsts, seconds = places_of(weight_ref, span, experts)
        pair = [jnp.zeros((rows, hidden_width), F32)] * 2
        for e in range(experts):
            gate, up = acts[e][:, :hidden_width] * scale, acts[e][:, hidden_width:] * scale
            weight = weight_ref[span, ROPE + e : ROPE + e + 1]
            hidden = gate / (1.0 + jnp.exp(-gate)) * up * weight
            hidden_ref[span, e * hidden_width : (e + 1) * hidden_width] = hidden.astype(BF16)
            pair = [jnp.where(firsts[e], hidden, pair[0]), jnp.where(seconds[e], hidden, pair[1])]
        pair_ref[span, :] = jnp.concatenate(pair, axis=1).astype(BF16)


def own_kernel(hidden_ref, down_ref, send_ref, keep_ref):
    place = lax.axis_index("tp")
    quarter = send_ref.shape[1]
    hidden = hidden_ref[...]
    for ref, mask in ((send_ref, 1), (keep_ref, 0)):
        cols = pl.ds(pl.multiple_of((place ^ mask) * quarter, LANES), quarter)
        ref[...] = dot(hidden, down_ref[:, cols])


def join_kernel(weight_ref, part_send_ref, part_keep_ref, *refs):
    send_ref, keep_ref = refs[-2:]
    count = (len(refs) - 2) // 3
    pairs, lows, highs = refs[:count], refs[count : 2 * count], refs[2 * count : -2]
    rows, quarter = send_ref.shape
    width = pairs[0].shape[1] // 2
    half_rows = lows[0].shape[0]
    experts = 2 * half_rows // width
    firsts, seconds = places_of(weight_ref, slice(0, rows), experts)
    send, keep = part_send_ref[...], part_keep_ref[...]
    core = lax.axis_index("tp") & 1
    for pair_ref, low_ref, high_ref in zip(pairs, lows, highs):
        pair = pair_ref[...]
        zero = jnp.zeros((rows, width), F32)
        one, two = pair[:, :width].astype(F32), pair[:, width:].astype(F32)
        hidden = jnp.concatenate(
            [jnp.where(firsts[e], one, jnp.where(seconds[e], two, zero)) for e in range(experts)], axis=1
        ).astype(BF16)
        for which, ref in enumerate((low_ref, high_ref)):
            part = hidden[:, which * half_rows : (which + 1) * half_rows]
            for bit in range(2):
                cols = pl.ds(pl.multiple_of((core ^ bit) * quarter, LANES), quarter)
                product = dot(part, ref[:, cols])
                if bit:
                    send = send + product
                else:
                    keep = keep + product
    send_ref[...] = send.astype(BF16)
    keep_ref[...] = keep.astype(BF16)


def start_copies(sources, targets, semaphores):
    copies = [
        pltpu.make_async_copy(source, target, semaphores.at[i])
        for i, (source, target) in enumerate(zip(sources, targets))
    ]
    for copy in copies:
        copy.start()
    return copies


def call(kernel, outs, inputs, fetched=(), kept=(), cuts=(), mib=12):
    whole = lambda ref: ref
    pieces = [(a, whole, a.shape) for a in kept] + list(cuts)
    kept = [a for a, _, _ in pieces]
    n_in, n_fetched, n_kept, n_out = len(inputs), len(fetched), len(kept), len(outs)

    def wrapped(*refs):
        refs = list(refs)
        take = lambda n: [refs.pop(0) for _ in range(n)]
        ins, sources, kept_sources = take(n_in), take(n_fetched), take(n_kept)
        results, kept_results, held = take(n_out), take(n_kept), take(n_fetched)
        first = start_copies(sources, held, refs[0]) if n_fetched else []
        kept_sources = [piece[1](source) for piece, source in zip(pieces, kept_sources)]
        second = start_copies(kept_sources, kept_results, refs[-1]) if n_kept else []
        for copy in first:
            copy.wait()
        kernel(*ins, *held, *results)
        for copy in second:
            copy.wait()

    semaphores = [pltpu.SemaphoreType.DMA((n,)) for n in (n_fetched, n_kept) if n]
    return pl.pallas_call(
        wrapped,
        out_shape=list(outs) + [held_shape(dims, a.dtype) for a, _, dims in pieces],
        in_specs=[VMEM] * n_in + [HBM] * (n_fetched + n_kept),
        out_specs=[VMEM] * (n_out + n_kept),
        scratch_shapes=[pltpu.VMEM(a.shape, a.dtype) for a in fetched] + semaphores,
        compiler_params=pltpu.CompilerParams(vmem_limit_bytes=mib * 2**20),
    )(
        *(pltpu.with_memory_space_constraint(a, pltpu.VMEM) for a in inputs),
        *(pltpu.with_memory_space_constraint(a, pltpu.HBM) for a in (*fetched, *kept)),
    )


def shape(dims, dtype=BF16):
    return jax.ShapeDtypeStruct(dims, dtype)


def held_shape(dims, dtype=BF16):
    return pltpu.VMEM(dims, dtype)


def body(
    query_wide,
    query_narrow,
    latent,
    rope_key,
    latent_norm_weight,
    broad_key_lift,
    broad_value_lift,
    slim_key_lift,
    slim_value_lift,
    out_wide,
    out_narrow,
    resid,
    ffn_gain,
    group_route,
    expert_pair,
    group_prob,
    expert_prob,
    gate_weight,
    up_weight,
    down_weight,
):
    tokens, rank = latent.shape
    groups = lax.axis_size("sp")
    tp_size = lax.axis_size("tp")
    place = lax.axis_index("sp")
    half = tokens // 2
    capacity = 2 * tokens // groups
    slots = groups * capacity
    model_width = resid.shape[1]
    quarter = model_width // tp_size
    route = group_route[None, :]
    far_masks = list(range(2, tp_size, 2))
    down_rows = down_weight[0].reshape(-1, model_width)

    def resid_cut(ref):
        return ref.at[:, pl.ds(pl.multiple_of(lax.axis_index("tp") * quarter, LANES), quarter)]

    def down_cut(mask, which, ref):
        rows, width = down_rows.shape[0] // 2, 2 * quarter
        upper = (lax.axis_index("tp") ^ mask) >> 1
        return ref.at[pl.ds(which * rows, rows), pl.ds(pl.multiple_of(upper * width, LANES), width)]

    query_pos = place * tokens + jnp.arange(tokens, dtype=jnp.int32)
    table = angles(query_pos, ROPE).T
    packed = held_shape((half, rank + LANES))
    tables = [jnp.cos(table), jnp.sin(table)]
    own, rest = call(
        pack_kernel, [packed, packed], tables,
        [latent, rope_key.T, latent_norm_weight[None, :], route, expert_pair.T, group_prob[None, :], expert_prob.T],
        mib=4,
    )

    strides = list(range(groups - 2, 0, -2))
    got = []
    for k in strides:
        got.append(exchange(own, "sp", k))
    beside = exchange(own, "sp", 1)
    across = [beside[None], exchange(beside, "sp", strides[-1])[None]]
    across.append(exchange(jnp.stack(got[:-1]), "sp", 1))
    column = [own, jnp.stack(got)]
    column_rest = [rest, exchange(column[1], "tp", 1)]
    across = jnp.concatenate(across)
    across_rest = exchange(across, "tp", 1)
    first_masks = [0] + strides
    second_masks = [1, strides[-1] ^ 1] + [k ^ 1 for k in strides[:-1]]
    heads = query_wide.shape[1] // (PLAIN_WIDTH_WIDE + ROPE) + query_narrow.shape[1] // (PLAIN_WIDTH_SLIM + ROPE)
    queries, *weights = call(
        query_kernel, [held_shape((heads, tokens, 2 * LANES))], tables, [query_wide, query_narrow],
        [broad_key_lift, broad_value_lift, slim_key_lift, slim_value_lift, out_wide, out_narrow],
        [
            (down_rows, functools.partial(down_cut, mask, which), (down_rows.shape[0] // 2, 2 * quarter))
            for mask in far_masks
            for which in range(2)
        ],
        mib=4,
    )
    lifts, out_weights, down_cuts = weights[:4], weights[4:6], weights[6:]
    down_low = [exchange(down_cuts[2 * i], "tp", mask) for i, mask in enumerate(far_masks)]
    down_high = [exchange(down_cuts[2 * i + 1], "tp", mask) for i, mask in enumerate(far_masks)]
    state_shape = [held_shape((heads, tokens, LANES), F32)] * 3
    state = call(functools.partial(first_kernel, first_masks), state_shape, [queries, *lifts, *column, *column_rest])
    state = call(
        functools.partial(second_kernel, second_masks), state_shape, [queries, *lifts, *state, across]
    )
    keep, send = call(
        functools.partial(third_kernel, second_masks), [held_shape((tp_size // 2, tokens, quarter))] * 2,
        [queries, *lifts, *state, *out_weights, across_rest],
    )
    slot_weights, hot, gate, up, down, gain, resid_cols = call(
        functools.partial(weights_kernel, first_masks + second_masks),
        [held_shape((slots, LANES), F32), held_shape((slots, tokens))],
        [route, *column, across, *column_rest, across_rest], [],
        [gate_weight[0], up_weight[0], down_rows, ffn_gain[None, :]],
        [(resid, resid_cut, (tokens, quarter))], mib=4,
    )

    received = exchange(send, "tp", 1)
    thin_rows = held_shape((tokens, quarter))
    stay, *sends = call(
        functools.partial(pair_kernel, far_masks), [thin_rows] * (1 + len(far_masks)), [keep, received], mib=4
    )
    came = [exchange(part, "tp", mask) for part, mask in zip(sends, far_masks)]
    stream_cols, placed = call(
        place_kernel, [thin_rows, held_shape((groups, capacity, quarter))],
        [resid_cols, hot, stay, *came], mib=4,
    )

    routed = lax.all_to_all(placed, "sp", split_axis=0, concat_axis=0, tiled=True)
    routed = routed.reshape(slots, quarter)
    part_rows = slots // 2
    far = []
    for first in (0, part_rows):
        far.append([exchange(routed[first : first + part_rows], "tp", mask) for mask in far_masks])
    near = exchange(routed, "tp", 1)
    experts, _, hidden_width = gate_weight[0].shape
    acts, square = call(
        functools.partial(near_kernel, [0, 1]),
        [held_shape((experts, slots, 2 * hidden_width), F32), held_shape((slots, LANES), F32)],
        [gain, gate, up, routed, near],
    )
    far_near = []
    for part in range(2):
        far_near.append([exchange(rows, "tp", 1) for rows in far[part]])
    hidden, pair = call(
        functools.partial(far_kernel, far_masks + [m | 1 for m in far_masks]),
        [held_shape((slots, experts * hidden_width)), held_shape((slots, 2 * hidden_width))],
        [gain, gate, up, slot_weights, acts, square, *far[0], *far_near[0], *far[1], *far_near[1]],
    )
    pairs = [exchange(pair, "tp", mask) for mask in far_masks]
    wide = held_shape((slots, quarter), F32)
    thin = held_shape((slots, quarter))
    part_send, part_keep = call(own_kernel, [wide, wide], [hidden, down])
    send, keep = call(join_kernel, [thin, thin], [slot_weights, part_send, part_keep, *pairs, *down_low, *down_high])
    received = exchange(send, "tp", 1)
    summed = (keep.astype(F32) + received.astype(F32)).astype(BF16)
    returned = lax.all_to_all(
        summed.reshape(groups, capacity, quarter), "sp", split_axis=0, concat_axis=0, tiled=True
    )
    return call(final_kernel, [shape((tokens, quarter))], [stream_cols, returned, hot], mib=4)[0]


def solution(mesh):
    placed = (
        P("sp", "tp"),
        P("sp", "tp"),
        P("sp", None),
        P("sp", None),
        P(),
        P(None, "tp"),
        P(None, "tp"),
        P(None, "tp"),
        P(None, "tp"),
        P("tp", None),
        P("tp", None),
        P("sp", None),
        P(),
        P("sp"),
        P("sp", None),
        P("sp"),
        P("sp", None),
        P("sp", None, None, "tp"),
        P("sp", None, None, "tp"),
        P("sp", None, "tp", None),
    )
    return jax.shard_map(body, mesh=mesh, in_specs=placed, out_specs=P("sp", "tp"), check_vma=False)
```

```python
import functools

import jax
import jax.numpy as jnp
from jax import lax
from jax.experimental import pallas as pl
from jax.experimental.pallas import tpu as pltpu
from jax.sharding import PartitionSpec as P


PLAIN_WIDTH_WIDE = 128
PLAIN_WIDTH_SLIM = 64
ROPE = 64
VALUE_WIDTH_WIDE = 128
VALUE_WIDTH_SLIM = 64
EPG = 4
LANES = 128

ROPE_BASE = 10000.0
EPSILON = 1e-06
MASKED = -1e30


F32 = jnp.float32
BF16 = jnp.bfloat16
VMEM = pl.BlockSpec(memory_space=pltpu.VMEM)
HBM = pl.BlockSpec(memory_space=pltpu.HBM)


def angles(positions, width):
    frequency = 1.0 / ROPE_BASE ** (jnp.arange(0, width, 2).astype(F32) / width)
    return positions.astype(F32)[:, None] * frequency[None, :]


def turn(values, cosine, sine, axis):
    first_half, second = jnp.split(values, 2, axis=axis)
    return jnp.concatenate(
        [first_half * cosine - second * sine, second * cosine + first_half * sine], axis=axis
    )


def exchange(values, axis, mask):
    size = lax.axis_size(axis)
    return lax.ppermute(values, axis, [(i, i ^ mask) for i in range(size)])


def dot(a, b):
    return jnp.dot(a, b, preferred_element_type=F32)


def dot_t(a, b):
    return lax.dot_general(a, b, (((1,), (1,)), ((), ())), preferred_element_type=F32)


def iota(shape, dim):
    return lax.broadcasted_iota(jnp.int32, shape, dim)


def prefix_count(rows):
    size = rows.shape[1]
    upto = (iota((size, size), 0) <= iota((size, size), 1)).astype(BF16)
    return dot(rows.astype(BF16), upto)


def pack_kernel(
    cos_ref, sin_ref, latent_ref, rope_ref, gain_ref, route_ref, pair_ref, group_ref, prob_ref,
    half_ref, rest_ref,
):
    rank = latent_ref.shape[1]
    half = half_ref.shape[0]
    tokens = latent_ref.shape[0]
    odd = (lax.axis_index("tp") & 1) == 1
    widened = latent_ref[...].astype(F32)
    scale = lax.rsqrt(jnp.mean(widened * widened, axis=-1, keepdims=True) + EPSILON)
    normed = (widened * scale * gain_ref[...]).astype(BF16)
    turned = turn(rope_ref[...].astype(F32), cos_ref[...], sin_ref[...], 0)
    shares = group_ref[...] * prob_ref[...] / jnp.sum(prob_ref[...], axis=0, keepdims=True)
    rows = iota((LANES - ROPE, tokens), 0)
    meta = jnp.where(rows == EPG, route_ref[...].astype(F32), 0.0)
    for expert in range(EPG):
        chosen = jnp.sum(jnp.where(pair_ref[...] == expert, shares, 0.0), axis=0, keepdims=True)
        meta = jnp.where(rows == expert, chosen, meta)
    tail = jnp.concatenate([turned, meta], axis=0).T.astype(BF16)
    half_ref[:, :rank] = jnp.where(odd, normed[half:], normed[:half])
    half_ref[:, rank:] = jnp.where(odd, tail[half:], tail[:half])
    rest_ref[:, :rank] = jnp.where(odd, normed[:half], normed[half:])
    rest_ref[:, rank:] = jnp.where(odd, tail[:half], tail[half:])


def query_kernel(cos_ref, sin_ref, wide_ref, slim_ref, out_ref):
    tokens = wide_ref.shape[0]
    heads_w = wide_ref.shape[1] // (PLAIN_WIDTH_WIDE + ROPE)
    heads_n = slim_ref.shape[1] // (PLAIN_WIDTH_SLIM + ROPE)
    spare = jnp.zeros((tokens, LANES - ROPE), F32)
    cosine, sine = cos_ref[...].T, sin_ref[...].T
    for h in range(heads_w + heads_n):
        wide = h < heads_w
        plain = PLAIN_WIDTH_WIDE if wide else PLAIN_WIDTH_SLIM
        start = (h if wide else h - heads_w) * (plain + ROPE)
        part = (wide_ref if wide else slim_ref)[:, start : start + plain + ROPE].astype(F32)
        pieces = [part[:, :plain], turn(part[:, plain:], cosine, sine, 1), spare]
        if not wide:
            before = (h - heads_w) * plain
            after = heads_n * plain - before - plain
            if before:
                pieces = [jnp.zeros((tokens, before), F32)] + pieces
            if after:
                pieces = pieces[:-2] + [jnp.zeros((tokens, after), F32)] + pieces[-2:]
        out_ref[h] = jnp.concatenate(pieces, axis=1).astype(BF16)


def pieces_of(refs):
    return [
        piece
        for ref in refs
        for piece in ([ref[...]] if len(ref.shape) == 2 else [ref[i] for i in range(ref.shape[0])])
    ]


def attend_body(queries, pieces, masks, mine, kw_ref, vw_ref, kn_ref, vn_ref, state):
    heads_w = kw_ref.shape[1] // PLAIN_WIDTH_WIDE
    heads_n = kn_ref.shape[1] // PLAIN_WIDTH_SLIM
    half = pieces[0].shape[0]
    tokens = queries[0].shape[0]
    rank = kw_ref.shape[0]
    place = lax.axis_index("sp")
    core = lax.axis_index("tp") & 1
    shift = half.bit_length() - 1
    step = 8
    for start in range(0, len(pieces), step):
        group = pieces[start : start + step]
        rows = len(group) * half
        lat = jnp.concatenate(group, axis=0)
        flat = lat[:, :rank]
        rot = lat[:, rank:]
        key_w = dot(flat, kw_ref[...]).astype(BF16)
        key_n = dot(flat, kn_ref[...]).astype(BF16)
        val_w = dot(flat, vw_ref[...]).astype(BF16)
        val_n = dot(flat, vn_ref[...]).astype(BF16)
        lane = iota((1, rows), 1)
        index = lane >> shift
        mask = jnp.zeros_like(lane)
        offset = jnp.zeros_like(lane)
        for i in range(len(group)):
            mask = jnp.where(index == i, masks[start + i], mask)
            offset = jnp.where(index == i, core if mine[start + i] else 1 - core, offset)
        key_pos = ((place ^ mask) * 2 + offset) * half + (lane & (half - 1))
        visible = iota((tokens, 1), 0) + place * tokens >= key_pos
        new_state = []
        for h in range(heads_w + heads_n):
            if h < heads_w:
                keys = key_w[:, h * PLAIN_WIDTH_WIDE : (h + 1) * PLAIN_WIDTH_WIDE]
                values = val_w[:, h * VALUE_WIDTH_WIDE : (h + 1) * VALUE_WIDTH_WIDE]
                scale = (PLAIN_WIDTH_WIDE + ROPE) ** (-0.5)
            else:
                keys = key_n
                values = val_n
                scale = (PLAIN_WIDTH_SLIM + ROPE) ** (-0.5)
            scores = dot_t(queries[h], jnp.concatenate([keys, rot], axis=1)) * scale
            scores = jnp.where(visible, scores, MASKED)
            peak = jnp.max(scores, axis=-1, keepdims=True)
            if state is not None:
                peak = jnp.maximum(peak, state[h][0])
            weights = jnp.exp(scores - peak)
            total = jnp.sum(weights, axis=-1, keepdims=True)
            acc = dot(weights.astype(BF16), values)
            if state is not None:
                keep = jnp.exp(state[h][0] - peak)
                total = total + state[h][1] * keep
                acc = acc + state[h][2] * keep
            new_state.append((peak, total, acc))
        state = new_state
    return state


def store_state(state, refs):
    peak_ref, total_ref, acc_ref = refs
    for h, (peak, total, acc) in enumerate(state):
        peak_ref[h] = jnp.broadcast_to(peak, peak_ref.shape[1:])
        total_ref[h] = jnp.broadcast_to(total, total_ref.shape[1:])
        acc_ref[h] = acc


def load_state(refs):
    peak_ref, total_ref, acc_ref = refs
    return [(peak_ref[h, :, :1], total_ref[h, :, :1], acc_ref[h]) for h in range(peak_ref.shape[0])]


def first_kernel(masks, q_ref, *refs):
    lifts, blocks = refs[:4], refs[4:-3]
    queries = [q_ref[h] for h in range(q_ref.shape[0])]
    mine = [True] * len(masks) + [False] * len(masks)
    store_state(attend_body(queries, pieces_of(blocks), masks * 2, mine, *lifts, None), refs[-3:])


def second_kernel(masks, q_ref, *refs):
    lifts, state_refs, blocks = refs[:4], refs[4:7], refs[7:-3]
    queries = [q_ref[h] for h in range(q_ref.shape[0])]
    state = attend_body(queries, pieces_of(blocks), masks, [True] * len(masks), *lifts, load_state(state_refs))
    store_state(state, refs[-3:])


def third_kernel(masks, q_ref, *refs):
    lifts, state_refs, (ow_ref, on_ref), blocks = refs[:4], refs[4:7], refs[7:9], refs[9:-3]
    send_ref, att_w_ref, att_n_ref = refs[-3:]
    queries = [q_ref[h] for h in range(q_ref.shape[0])]
    heads = len(queries)
    heads_w = lifts[0].shape[1] // PLAIN_WIDTH_WIDE
    state = attend_body(queries, pieces_of(blocks), masks, [False] * len(masks), *lifts, load_state(state_refs))
    done = [acc / total for _, total, acc in state]
    att_w = jnp.concatenate(done[:heads_w], axis=1).astype(BF16)
    slim = done[heads_w]
    for h in range(1, heads - heads_w):
        lane = iota(slim.shape, 1)
        slim = jnp.where(lane >= h * VALUE_WIDTH_SLIM, done[heads_w + h], slim)
    att_n = slim.astype(BF16)
    att_w_ref[...] = att_w
    att_n_ref[...] = att_n
    project(att_w, att_n, ow_ref, on_ref, send_ref, 1 - (lax.axis_index("tp") & 1))


def project(att_w, att_n, ow_ref, on_ref, out_ref, bit):
    pieces, _, quarter = out_ref.shape
    for piece in range(pieces):
        cols = pl.ds(pl.multiple_of((2 * piece + bit) * quarter, LANES), quarter)
        out_ref[piece] = (dot(att_w, ow_ref[:, cols]) + dot(att_n, on_ref[:, cols])).astype(BF16)


def keep_kernel(att_w_ref, att_n_ref, ow_ref, on_ref, keep_ref):
    project(att_w_ref[...], att_n_ref[...], ow_ref, on_ref, keep_ref, lax.axis_index("tp") & 1)


def slots_of(route, groups, capacity):
    tokens = route.shape[1]
    member = (iota((groups, tokens), 0) == route).astype(F32)
    rank_of = jnp.sum(prefix_count(member) * member, axis=0, keepdims=True).astype(jnp.int32) - 1
    slot = route * capacity + rank_of
    return (iota((groups * capacity, tokens), 0) == slot).astype(BF16)


def weights_kernel(masks, route_ref, *refs):
    refs, hot_ref = refs[:-1], refs[-1]
    out_ref = refs[-1]
    count = (len(refs) - 1) // 2
    mine_all, other_all = pieces_of(refs[:count]), pieces_of(refs[count:-1])
    half, width = mine_all[0].shape
    place = lax.axis_index("sp")
    odd = (lax.axis_index("tp") & 1) == 1
    capacity = out_ref.shape[0] // len(mine_all)
    base = width - LANES
    hot_ref[...] = slots_of(route_ref[...], len(mine_all), capacity)
    for mask, mine, other in zip(masks, mine_all, other_all):
        mine, other = mine[:, base:], other[:, base:]
        data = jnp.concatenate(
            [jnp.where(odd, other, mine), jnp.where(odd, mine, other)], axis=0
        )
        route = data.astype(F32).T[ROPE + EPG : ROPE + EPG + 1]
        here = (route == place.astype(F32)).astype(F32)
        order = prefix_count(here) - 1.0
        hot = jnp.where((iota((capacity, 2 * half), 0).astype(F32) == order) & (here > 0), 1.0, 0.0)
        start = pl.multiple_of((place ^ mask) * capacity, capacity)
        out_ref[pl.ds(start, capacity), :] = dot(hot.astype(BF16), data)


def pair_kernel(masks, keep_ref, got_ref, stay_ref, *send_refs):
    upper = lax.axis_index("tp") >> 1
    for ref, mask in zip((stay_ref, *send_refs), [0] + masks):
        piece = upper ^ (mask >> 1)
        ref[...] = (keep_ref[piece].astype(F32) + got_ref[piece].astype(F32)).astype(BF16)


def place_kernel(resid_ref, hot_ref, *refs):
    stream_ref, placed_ref = refs[-2:]
    stream = resid_ref[...].astype(F32)
    for ref in refs[:-2]:
        stream = stream + ref[...].astype(F32)
    stream = stream.astype(BF16)
    stream_ref[...] = stream
    placed_ref[...] = dot(hot_ref[...], stream).astype(BF16).reshape(placed_ref.shape)


def final_kernel(stream_ref, back_ref, hot_ref, out_ref):
    groups, capacity, quarter = back_ref.shape
    rows = back_ref[...].reshape(groups * capacity, quarter)
    moe = lax.dot_general(hot_ref[...], rows, (((0,), (0,)), ((), ())), preferred_element_type=F32)
    out_ref[...] = (stream_ref[...].astype(F32) + moe).astype(BF16)


def expand_part(masks, gain_ref, gate_ref, up_ref, parts, acts, square):
    quarter = parts[0].shape[1]
    place = lax.axis_index("tp")
    for mask, part in zip(masks, parts):
        cols = pl.ds(pl.multiple_of((place ^ mask) * quarter, LANES), quarter)
        rows = part[...].astype(F32)
        square = square + jnp.sum(rows * rows, axis=-1, keepdims=True)
        scaled = (rows * gain_ref[:, cols]).astype(BF16)
        for e in range(len(acts)):
            both = jnp.concatenate([gate_ref[e, cols, :], up_ref[e, cols, :]], axis=1)
            acts[e] = acts[e] + dot(scaled, both)
    return square


def near_kernel(masks, gain_ref, gate_ref, up_ref, *refs):
    act_ref, square_ref = refs[-2:]
    acts = [0.0] * act_ref.shape[0]
    square = expand_part(masks, gain_ref, gate_ref, up_ref, refs[:-2], acts, 0.0)
    for e, act in enumerate(acts):
        act_ref[e] = act
    square_ref[...] = jnp.broadcast_to(square, square_ref.shape)


def places_of(weight_ref, span, experts):
    firsts, seconds = [], []
    seen = 0.0
    for e in range(experts):
        chosen = jnp.where(weight_ref[span, ROPE + e : ROPE + e + 1] != 0.0, 1.0, 0.0)
        firsts.append((chosen > 0.0) & (seen == 0.0))
        seconds.append((chosen > 0.0) & (seen == 1.0))
        seen = seen + chosen
    return firsts, seconds


def far_kernel(masks, first, gain_ref, gate_ref, up_ref, weight_ref, act_ref, square_ref, *refs):
    hidden_ref, pair_ref = refs[-2:]
    experts, model_width, hidden_width = gate_ref.shape
    rows = hidden_ref.shape[0]
    span = slice(first, first + rows)
    acts = [act_ref[e, span, :] for e in range(experts)]
    square = expand_part(masks, gain_ref, gate_ref, up_ref, refs[:-2], acts, square_ref[span, :1])
    scale = lax.rsqrt(square / model_width + EPSILON)
    firsts, seconds = places_of(weight_ref, span, experts)
    pair = [jnp.zeros((rows, hidden_width), F32)] * 2
    for e in range(experts):
        gate, up = acts[e][:, :hidden_width] * scale, acts[e][:, hidden_width:] * scale
        weight = weight_ref[span, ROPE + e : ROPE + e + 1]
        hidden = gate / (1.0 + jnp.exp(-gate)) * up * weight
        hidden_ref[:, e * hidden_width : (e + 1) * hidden_width] = hidden.astype(BF16)
        pair = [jnp.where(firsts[e], hidden, pair[0]), jnp.where(seconds[e], hidden, pair[1])]
    pair_ref[...] = jnp.concatenate(pair, axis=1).astype(BF16)


def own_kernel(down_ref, *refs):
    send_ref, keep_ref = refs[-2:]
    place = lax.axis_index("tp")
    quarter = send_ref.shape[1]
    hidden = jnp.concatenate([ref[...] for ref in refs[:-2]], axis=0)
    for ref, mask in ((send_ref, 1), (keep_ref, 0)):
        cols = pl.ds(pl.multiple_of((place ^ mask) * quarter, LANES), quarter)
        ref[...] = dot(hidden, down_ref[:, cols])


def join_kernel(count, first, weight_ref, part_send_ref, part_keep_ref, *refs):
    send_ref, keep_ref = refs[-2:]
    lows, highs, pairs = refs[:count], refs[count : 2 * count], refs[2 * count : -2]
    rows, quarter = send_ref.shape
    width = pairs[0].shape[1] // 2
    half_rows = lows[0].shape[0]
    experts = 2 * half_rows // width
    span = slice(first, first + rows)
    firsts, seconds = places_of(weight_ref, span, experts)
    send, keep = part_send_ref[span, :], part_keep_ref[span, :]
    core = lax.axis_index("tp") & 1
    for i in range(count):
        pair = pairs[i][...]
        zero = jnp.zeros((rows, width), F32)
        one, two = pair[:, :width].astype(F32), pair[:, width:].astype(F32)
        hidden = jnp.concatenate(
            [jnp.where(firsts[e], one, jnp.where(seconds[e], two, zero)) for e in range(experts)], axis=1
        ).astype(BF16)
        for bit in range(2):
            cols = pl.ds(pl.multiple_of((core ^ bit) * quarter, LANES), quarter)
            product = dot(hidden, jnp.concatenate([lows[i][:, cols], highs[i][:, cols]], axis=0))
            if bit:
                send = send + product
            else:
                keep = keep + product
    send_ref[...] = send.astype(BF16)
    keep_ref[...] = keep.astype(BF16)


def start_copies(sources, targets, semaphores):
    copies = [
        pltpu.make_async_copy(source, target, semaphores.at[i])
        for i, (source, target) in enumerate(zip(sources, targets))
    ]
    for copy in copies:
        copy.start()
    return copies


def call(kernel, outs, inputs, fetched=(), kept=(), cuts=(), mib=12):
    whole = lambda ref: ref
    pieces = [(a, whole, a.shape) for a in kept] + list(cuts)
    kept = [a for a, _, _ in pieces]
    n_in, n_fetched, n_kept, n_out = len(inputs), len(fetched), len(kept), len(outs)

    def wrapped(*refs):
        refs = list(refs)
        take = lambda n: [refs.pop(0) for _ in range(n)]
        ins, sources, kept_sources = take(n_in), take(n_fetched), take(n_kept)
        results, kept_results, held = take(n_out), take(n_kept), take(n_fetched)
        first = start_copies(sources, held, refs[0]) if n_fetched else []
        kept_sources = [piece[1](source) for piece, source in zip(pieces, kept_sources)]
        second = start_copies(kept_sources, kept_results, refs[-1]) if n_kept else []
        for copy in first:
            copy.wait()
        kernel(*ins, *held, *results)
        for copy in second:
            copy.wait()

    semaphores = [pltpu.SemaphoreType.DMA((n,)) for n in (n_fetched, n_kept) if n]
    return pl.pallas_call(
        wrapped,
        out_shape=list(outs) + [held_shape(dims, a.dtype) for a, _, dims in pieces],
        in_specs=[VMEM] * n_in + [HBM] * (n_fetched + n_kept),
        out_specs=[VMEM] * (n_out + n_kept),
        scratch_shapes=[pltpu.VMEM(a.shape, a.dtype) for a in fetched] + semaphores,
        compiler_params=pltpu.CompilerParams(vmem_limit_bytes=mib * 2**20),
    )(
        *(pltpu.with_memory_space_constraint(a, pltpu.VMEM) for a in inputs),
        *(pltpu.with_memory_space_constraint(a, pltpu.HBM) for a in (*fetched, *kept)),
    )


def shape(dims, dtype=BF16):
    return jax.ShapeDtypeStruct(dims, dtype)


def held_shape(dims, dtype=BF16):
    return pltpu.VMEM(dims, dtype)


def body(
    query_wide,
    query_narrow,
    latent,
    rope_key,
    latent_norm_weight,
    broad_key_lift,
    broad_value_lift,
    slim_key_lift,
    slim_value_lift,
    out_wide,
    out_narrow,
    resid,
    ffn_gain,
    group_route,
    expert_pair,
    group_prob,
    expert_prob,
    gate_weight,
    up_weight,
    down_weight,
):
    tokens, rank = latent.shape
    groups = lax.axis_size("sp")
    tp_size = lax.axis_size("tp")
    place = lax.axis_index("sp")
    half = tokens // 2
    capacity = 2 * tokens // groups
    slots = groups * capacity
    model_width = resid.shape[1]
    quarter = model_width // tp_size
    route = group_route[None, :]
    far_masks = list(range(2, tp_size, 2))
    down_rows = down_weight[0].reshape(-1, model_width)

    def resid_cut(ref):
        return ref.at[:, pl.ds(pl.multiple_of(lax.axis_index("tp") * quarter, LANES), quarter)]

    def down_cut(mask, which, ref):
        rows, width = down_rows.shape[0] // 2, 2 * quarter
        upper = (lax.axis_index("tp") ^ mask) >> 1
        return ref.at[pl.ds(which * rows, rows), pl.ds(pl.multiple_of(upper * width, LANES), width)]

    query_pos = place * tokens + jnp.arange(tokens, dtype=jnp.int32)
    table = angles(query_pos, ROPE).T
    packed = held_shape((half, rank + LANES))
    tables = [jnp.cos(table), jnp.sin(table)]
    own, rest = call(
        pack_kernel, [packed, packed], tables,
        [latent, rope_key.T, latent_norm_weight[None, :], route, expert_pair.T, group_prob[None, :], expert_prob.T],
        mib=4,
    )

    strides = list(range(groups - 2, 0, -2))
    got = []
    for k in strides:
        got.append(exchange(own, "sp", k))
    beside = exchange(own, "sp", 1)
    across = [beside[None], exchange(beside, "sp", strides[-1])[None]]
    across.append(exchange(jnp.stack(got[:-1]), "sp", 1))
    column = [own, jnp.stack(got)]
    column_rest = [rest, exchange(column[1], "tp", 1)]
    across = jnp.concatenate(across)
    across_rest = exchange(across, "tp", 1)
    first_masks = [0] + strides
    second_masks = [1, strides[-1] ^ 1] + [k ^ 1 for k in strides[:-1]]
    heads = query_wide.shape[1] // (PLAIN_WIDTH_WIDE + ROPE) + query_narrow.shape[1] // (PLAIN_WIDTH_SLIM + ROPE)
    queries, *weights = call(
        query_kernel, [held_shape((heads, tokens, 2 * LANES))], tables, [query_wide, query_narrow],
        [broad_key_lift, broad_value_lift, slim_key_lift, slim_value_lift, out_wide, out_narrow],
        [
            (down_rows, functools.partial(down_cut, mask, which), (down_rows.shape[0] // 2, 2 * quarter))
            for mask in far_masks
            for which in range(2)
        ],
        mib=4,
    )
    lifts, out_weights, down_cuts = weights[:4], weights[4:6], weights[6:]
    down_low = [exchange(down_cuts[2 * i], "tp", mask) for i, mask in enumerate(far_masks)]
    down_high = [exchange(down_cuts[2 * i + 1], "tp", mask) for i, mask in enumerate(far_masks)]
    state_shape = [held_shape((heads, tokens, LANES), F32)] * 3
    state = call(functools.partial(first_kernel, first_masks), state_shape, [queries, *lifts, *column, *column_rest])
    state = call(
        functools.partial(second_kernel, second_masks), state_shape, [queries, *lifts, *state, across]
    )
    pieces_shape = held_shape((tp_size // 2, tokens, quarter))
    send, att_w, att_n = call(
        functools.partial(third_kernel, second_masks),
        [pieces_shape, held_shape((tokens, out_wide.shape[0])), held_shape((tokens, out_narrow.shape[0]))],
        [queries, *lifts, *state, *out_weights, across_rest],
    )
    (keep,) = call(keep_kernel, [pieces_shape], [att_w, att_n, *out_weights], mib=4)
    slot_weights, hot, gate, up, down, gain, resid_cols = call(
        functools.partial(weights_kernel, first_masks + second_masks),
        [held_shape((slots, LANES), F32), held_shape((slots, tokens))],
        [route, *column, across, *column_rest, across_rest], [],
        [gate_weight[0], up_weight[0], down_rows, ffn_gain[None, :]],
        [(resid, resid_cut, (tokens, quarter))], mib=4,
    )

    received = exchange(send, "tp", 1)
    thin_rows = held_shape((tokens, quarter))
    stay, *sends = call(
        functools.partial(pair_kernel, far_masks), [thin_rows] * (1 + len(far_masks)), [keep, received], mib=4
    )
    came = [exchange(part, "tp", mask) for part, mask in zip(sends, far_masks)]
    stream_cols, placed = call(
        place_kernel, [thin_rows, held_shape((groups, capacity, quarter))],
        [resid_cols, hot, stay, *came], mib=4,
    )

    routed = lax.all_to_all(placed, "sp", split_axis=0, concat_axis=0, tiled=True)
    routed = routed.reshape(slots, quarter)
    part_rows = slots // 2
    far = []
    for first in (0, part_rows):
        far.append([exchange(routed[first : first + part_rows], "tp", mask) for mask in far_masks])
    near = exchange(routed, "tp", 1)
    experts, _, hidden_width = gate_weight[0].shape
    acts, square = call(
        functools.partial(near_kernel, [0, 1]),
        [held_shape((experts, slots, 2 * hidden_width), F32), held_shape((slots, LANES), F32)],
        [gain, gate, up, routed, near],
    )
    hidden, pairs = [], []
    for part in range(2):
        far_near = [exchange(rows, "tp", 1) for rows in far[part]]
        units, pair = call(
            functools.partial(far_kernel, far_masks + [m | 1 for m in far_masks], part * part_rows),
            [held_shape((part_rows, experts * hidden_width)), held_shape((part_rows, 2 * hidden_width))],
            [gain, gate, up, slot_weights, acts, square, *far[part], *far_near],
        )
        hidden.append(units)
        pairs.append([exchange(pair, "tp", mask) for mask in far_masks])
    wide = held_shape((slots, quarter), F32)
    thin = held_shape((part_rows, quarter))
    part_send, part_keep = call(own_kernel, [wide, wide], [down, *hidden])
    summed = []
    for part in range(2):
        send, keep = call(
            functools.partial(join_kernel, len(far_masks), part * part_rows), [thin, thin],
            [slot_weights, part_send, part_keep, *down_low, *down_high, *pairs[part]],
        )
        received = exchange(send, "tp", 1)
        summed.append((keep.astype(F32) + received.astype(F32)).astype(BF16))
    returned = lax.all_to_all(
        jnp.concatenate(summed).reshape(groups, capacity, quarter), "sp", split_axis=0, concat_axis=0, tiled=True
    )
    return call(final_kernel, [shape((tokens, quarter))], [stream_cols, returned, hot], mib=4)[0]


def solution(mesh):
    placed = (
        P("sp", "tp"),
        P("sp", "tp"),
        P("sp", None),
        P("sp", None),
        P(),
        P(None, "tp"),
        P(None, "tp"),
        P(None, "tp"),
        P(None, "tp"),
        P("tp", None),
        P("tp", None),
        P("sp", None),
        P(),
        P("sp"),
        P("sp", None),
        P("sp"),
        P("sp", None),
        P("sp", None, None, "tp"),
        P("sp", None, None, "tp"),
        P("sp", None, "tp", None),
    )
    return jax.shard_map(body, mesh=mesh, in_specs=placed, out_specs=P("sp", "tp"), check_vma=False)
```

```python
import functools

import jax
import jax.numpy as jnp
from jax import lax
from jax.experimental import pallas as pl
from jax.experimental.pallas import tpu as pltpu
from jax.sharding import PartitionSpec as P


PLAIN_WIDTH_WIDE = 128
PLAIN_WIDTH_SLIM = 64
ROPE = 64
VALUE_WIDTH_WIDE = 128
VALUE_WIDTH_SLIM = 64
EPG = 4
LANES = 128

ROPE_BASE = 10000.0
EPSILON = 1e-06
MASKED = -1e30


F32 = jnp.float32
BF16 = jnp.bfloat16
VMEM = pl.BlockSpec(memory_space=pltpu.VMEM)
HBM = pl.BlockSpec(memory_space=pltpu.HBM)


def angles(positions, width):
    frequency = 1.0 / ROPE_BASE ** (jnp.arange(0, width, 2).astype(F32) / width)
    return positions.astype(F32)[:, None] * frequency[None, :]


def turn(values, cosine, sine, axis):
    first_half, second = jnp.split(values, 2, axis=axis)
    return jnp.concatenate(
        [first_half * cosine - second * sine, second * cosine + first_half * sine], axis=axis
    )


def exchange(values, axis, mask):
    size = lax.axis_size(axis)
    return lax.ppermute(values, axis, [(i, i ^ mask) for i in range(size)])


def dot(a, b):
    return jnp.dot(a, b, preferred_element_type=F32)


def dot_t(a, b):
    return lax.dot_general(a, b, (((1,), (1,)), ((), ())), preferred_element_type=F32)


def iota(shape, dim):
    return lax.broadcasted_iota(jnp.int32, shape, dim)


def prefix_count(rows):
    size = rows.shape[1]
    upto = (iota((size, size), 0) <= iota((size, size), 1)).astype(BF16)
    return dot(rows.astype(BF16), upto)


def pack_kernel(
    cos_ref, sin_ref, latent_ref, rope_ref, gain_ref, route_ref, pair_ref, group_ref, prob_ref,
    half_ref, rest_ref,
):
    rank = latent_ref.shape[1]
    half = half_ref.shape[0]
    tokens = latent_ref.shape[0]
    odd = (lax.axis_index("tp") & 1) == 1
    widened = latent_ref[...].astype(F32)
    scale = lax.rsqrt(jnp.mean(widened * widened, axis=-1, keepdims=True) + EPSILON)
    normed = (widened * scale * gain_ref[...]).astype(BF16)
    turned = turn(rope_ref[...].astype(F32), cos_ref[...], sin_ref[...], 0)
    shares = group_ref[...] * prob_ref[...] / jnp.sum(prob_ref[...], axis=0, keepdims=True)
    rows = iota((LANES - ROPE, tokens), 0)
    meta = jnp.where(rows == EPG, route_ref[...].astype(F32), 0.0)
    for expert in range(EPG):
        chosen = jnp.sum(jnp.where(pair_ref[...] == expert, shares, 0.0), axis=0, keepdims=True)
        meta = jnp.where(rows == expert, chosen, meta)
    tail = jnp.concatenate([turned, meta], axis=0).T.astype(BF16)
    half_ref[:, :rank] = jnp.where(odd, normed[half:], normed[:half])
    half_ref[:, rank:] = jnp.where(odd, tail[half:], tail[:half])
    rest_ref[:, :rank] = jnp.where(odd, normed[:half], normed[half:])
    rest_ref[:, rank:] = jnp.where(odd, tail[:half], tail[half:])


def query_kernel(cos_ref, sin_ref, wide_ref, slim_ref, out_ref):
    tokens = wide_ref.shape[0]
    heads_w = wide_ref.shape[1] // (PLAIN_WIDTH_WIDE + ROPE)
    heads_n = slim_ref.shape[1] // (PLAIN_WIDTH_SLIM + ROPE)
    spare = jnp.zeros((tokens, LANES - ROPE), F32)
    cosine, sine = cos_ref[...].T, sin_ref[...].T
    for h in range(heads_w + heads_n):
        wide = h < heads_w
        plain = PLAIN_WIDTH_WIDE if wide else PLAIN_WIDTH_SLIM
        start = (h if wide else h - heads_w) * (plain + ROPE)
        part = (wide_ref if wide else slim_ref)[:, start : start + plain + ROPE].astype(F32)
        pieces = [part[:, :plain], turn(part[:, plain:], cosine, sine, 1), spare]
        if not wide:
            before = (h - heads_w) * plain
            after = heads_n * plain - before - plain
            if before:
                pieces = [jnp.zeros((tokens, before), F32)] + pieces
            if after:
                pieces = pieces[:-2] + [jnp.zeros((tokens, after), F32)] + pieces[-2:]
        out_ref[h] = jnp.concatenate(pieces, axis=1).astype(BF16)


def pieces_of(refs):
    return [
        piece
        for ref in refs
        for piece in ([ref[...]] if len(ref.shape) == 2 else [ref[i] for i in range(ref.shape[0])])
    ]


def attend_body(queries, pieces, masks, mine, kw_ref, vw_ref, kn_ref, vn_ref, state):
    heads_w = kw_ref.shape[1] // PLAIN_WIDTH_WIDE
    heads_n = kn_ref.shape[1] // PLAIN_WIDTH_SLIM
    half = pieces[0].shape[0]
    tokens = queries[0].shape[0]
    rank = kw_ref.shape[0]
    place = lax.axis_index("sp")
    core = lax.axis_index("tp") & 1
    shift = half.bit_length() - 1
    step = 8
    for start in range(0, len(pieces), step):
        group = pieces[start : start + step]
        rows = len(group) * half
        lat = jnp.concatenate(group, axis=0)
        flat = lat[:, :rank]
        rot = lat[:, rank:]
        key_w = dot(flat, kw_ref[...]).astype(BF16)
        key_n = dot(flat, kn_ref[...]).astype(BF16)
        val_w = dot(flat, vw_ref[...]).astype(BF16)
        val_n = dot(flat, vn_ref[...]).astype(BF16)
        lane = iota((1, rows), 1)
        index = lane >> shift
        mask = jnp.zeros_like(lane)
        offset = jnp.zeros_like(lane)
        for i in range(len(group)):
            mask = jnp.where(index == i, masks[start + i], mask)
            offset = jnp.where(index == i, core if mine[start + i] else 1 - core, offset)
        key_pos = ((place ^ mask) * 2 + offset) * half + (lane & (half - 1))
        visible = iota((tokens, 1), 0) + place * tokens >= key_pos
        scored = []
        for h in range(heads_w + heads_n):
            if h < heads_w:
                keys = key_w[:, h * PLAIN_WIDTH_WIDE : (h + 1) * PLAIN_WIDTH_WIDE]
                scale = (PLAIN_WIDTH_WIDE + ROPE) ** (-0.5)
            else:
                keys = key_n
                scale = (PLAIN_WIDTH_SLIM + ROPE) ** (-0.5)
            scores = dot_t(queries[h], jnp.concatenate([keys, rot], axis=1)) * scale
            scored.append(jnp.where(visible, scores, MASKED))
        peaks = [jnp.max(scores, axis=-1, keepdims=True) for scores in scored]
        if state is not None:
            peaks = [jnp.maximum(peak, state[h][0]) for h, peak in enumerate(peaks)]
        weighed = [jnp.exp(scores - peak) for scores, peak in zip(scored, peaks)]
        totals = [jnp.sum(weights, axis=-1, keepdims=True) for weights in weighed]
        accs = []
        for h, weights in enumerate(weighed):
            values = val_w[:, h * VALUE_WIDTH_WIDE : (h + 1) * VALUE_WIDTH_WIDE] if h < heads_w else val_n
            accs.append(dot(weights.astype(BF16), values))
        if state is not None:
            keeps = [jnp.exp(state[h][0] - peak) for h, peak in enumerate(peaks)]
            totals = [total + state[h][1] * keeps[h] for h, total in enumerate(totals)]
            accs = [acc + state[h][2] * keeps[h] for h, acc in enumerate(accs)]
        state = list(zip(peaks, totals, accs))
    return state


def store_state(state, refs):
    peak_ref, total_ref, acc_ref = refs
    for h, (peak, total, acc) in enumerate(state):
        peak_ref[h] = jnp.broadcast_to(peak, peak_ref.shape[1:])
        total_ref[h] = jnp.broadcast_to(total, total_ref.shape[1:])
        acc_ref[h] = acc


def merged(states):
    peak = functools.reduce(jnp.maximum, [part[0] for part in states])
    factors = [jnp.exp(part[0] - peak) for part in states]
    total = sum(part[1] * factor for part, factor in zip(states, factors))
    return sum(part[2] * factor for part, factor in zip(states, factors)) / total


def first_kernel(masks, q_ref, *refs):
    lifts, blocks = refs[:4], refs[4:-3]
    queries = [q_ref[h] for h in range(q_ref.shape[0])]
    mine = [True] * len(masks) + [False] * len(masks)
    store_state(attend_body(queries, pieces_of(blocks), masks * 2, mine, *lifts, None), refs[-3:])


def second_kernel(masks, q_ref, *refs):
    lifts, blocks = refs[:4], refs[4:-3]
    queries = [q_ref[h] for h in range(q_ref.shape[0])]
    state = attend_body(queries, pieces_of(blocks), masks, [True] * len(masks), *lifts, None)
    store_state(state, refs[-3:])


def third_kernel(masks, q_ref, *refs):
    lifts, state_refs, (ow_ref, on_ref), blocks = refs[:4], (refs[4:7], refs[7:10]), refs[10:12], refs[12:-3]
    send_ref, att_w_ref, att_n_ref = refs[-3:]
    queries = [q_ref[h] for h in range(q_ref.shape[0])]
    heads = len(queries)
    heads_w = lifts[0].shape[1] // PLAIN_WIDTH_WIDE
    state = attend_body(queries, pieces_of(blocks), masks, [False] * len(masks), *lifts, None)
    done = []
    for h, (peak, total, acc) in enumerate(state):
        fresh = (jnp.broadcast_to(peak, acc.shape), jnp.broadcast_to(total, acc.shape), acc)
        done.append(merged([fresh] + [tuple(ref[h] for ref in held) for held in state_refs]))
    att_w = jnp.concatenate(done[:heads_w], axis=1).astype(BF16)
    slim = done[heads_w]
    for h in range(1, heads - heads_w):
        lane = iota(slim.shape, 1)
        slim = jnp.where(lane >= h * VALUE_WIDTH_SLIM, done[heads_w + h], slim)
    att_n = slim.astype(BF16)
    att_w_ref[...] = att_w
    att_n_ref[...] = att_n
    project(att_w, att_n, ow_ref, on_ref, send_ref, 1 - (lax.axis_index("tp") & 1))


def project(att_w, att_n, ow_ref, on_ref, out_ref, bit):
    pieces, _, quarter = out_ref.shape
    for piece in range(pieces):
        cols = pl.ds(pl.multiple_of((2 * piece + bit) * quarter, LANES), quarter)
        out_ref[piece] = (dot(att_w, ow_ref[:, cols]) + dot(att_n, on_ref[:, cols])).astype(BF16)


def keep_kernel(att_w_ref, att_n_ref, ow_ref, on_ref, keep_ref):
    project(att_w_ref[...], att_n_ref[...], ow_ref, on_ref, keep_ref, lax.axis_index("tp") & 1)


def slots_of(route, groups, capacity):
    tokens = route.shape[1]
    member = (iota((groups, tokens), 0) == route).astype(F32)
    rank_of = jnp.sum(prefix_count(member) * member, axis=0, keepdims=True).astype(jnp.int32) - 1
    slot = route * capacity + rank_of
    return (iota((groups * capacity, tokens), 0) == slot).astype(BF16)


def weights_kernel(masks, route_ref, *refs):
    refs, hot_ref = refs[:-1], refs[-1]
    out_ref = refs[-1]
    count = (len(refs) - 1) // 2
    mine_all, other_all = pieces_of(refs[:count]), pieces_of(refs[count:-1])
    half, width = mine_all[0].shape
    place = lax.axis_index("sp")
    odd = (lax.axis_index("tp") & 1) == 1
    capacity = out_ref.shape[0] // len(mine_all)
    base = width - LANES
    hot_ref[...] = slots_of(route_ref[...], len(mine_all), capacity)
    for mask, mine, other in zip(masks, mine_all, other_all):
        mine, other = mine[:, base:], other[:, base:]
        data = jnp.concatenate(
            [jnp.where(odd, other, mine), jnp.where(odd, mine, other)], axis=0
        )
        route = data.astype(F32).T[ROPE + EPG : ROPE + EPG + 1]
        here = (route == place.astype(F32)).astype(F32)
        order = prefix_count(here) - 1.0
        hot = jnp.where((iota((capacity, 2 * half), 0).astype(F32) == order) & (here > 0), 1.0, 0.0)
        start = pl.multiple_of((place ^ mask) * capacity, capacity)
        out_ref[pl.ds(start, capacity), :] = dot(hot.astype(BF16), data)


def pair_kernel(masks, keep_ref, got_ref, stay_ref, *send_refs):
    upper = lax.axis_index("tp") >> 1
    for ref, mask in zip((stay_ref, *send_refs), [0] + masks):
        piece = upper ^ (mask >> 1)
        ref[...] = (keep_ref[piece].astype(F32) + got_ref[piece].astype(F32)).astype(BF16)


def place_kernel(resid_ref, hot_ref, *refs):
    stream_ref, placed_ref = refs[-2:]
    stream = resid_ref[...].astype(F32)
    for ref in refs[:-2]:
        stream = stream + ref[...].astype(F32)
    stream = stream.astype(BF16)
    stream_ref[...] = stream
    placed_ref[...] = dot(hot_ref[...], stream).astype(BF16).reshape(placed_ref.shape)


def final_kernel(stream_ref, back_ref, hot_ref, out_ref):
    groups, capacity, quarter = back_ref.shape
    rows = back_ref[...].reshape(groups * capacity, quarter)
    moe = lax.dot_general(hot_ref[...], rows, (((0,), (0,)), ((), ())), preferred_element_type=F32)
    out_ref[...] = (stream_ref[...].astype(F32) + moe).astype(BF16)


def expand_part(masks, gain_ref, gate_ref, up_ref, parts, acts, square):
    quarter = parts[0].shape[1]
    place = lax.axis_index("tp")
    for mask, part in zip(masks, parts):
        cols = pl.ds(pl.multiple_of((place ^ mask) * quarter, LANES), quarter)
        rows = part[...].astype(F32)
        square = square + jnp.sum(rows * rows, axis=-1, keepdims=True)
        scaled = (rows * gain_ref[:, cols]).astype(BF16)
        for e in range(len(acts)):
            both = jnp.concatenate([gate_ref[e, cols, :], up_ref[e, cols, :]], axis=1)
            acts[e] = acts[e] + dot(scaled, both)
    return square


def near_kernel(masks, gain_ref, gate_ref, up_ref, *refs):
    act_ref, square_ref = refs[-2:]
    acts = [0.0] * act_ref.shape[0]
    square = expand_part(masks, gain_ref, gate_ref, up_ref, refs[:-2], acts, 0.0)
    for e, act in enumerate(acts):
        act_ref[e] = act
    square_ref[...] = jnp.broadcast_to(square, square_ref.shape)


def places_of(weight_ref, span, experts):
    firsts, seconds = [], []
    seen = 0.0
    for e in range(experts):
        chosen = jnp.where(weight_ref[span, ROPE + e : ROPE + e + 1] != 0.0, 1.0, 0.0)
        firsts.append((chosen > 0.0) & (seen == 0.0))
        seconds.append((chosen > 0.0) & (seen == 1.0))
        seen = seen + chosen
    return firsts, seconds


def far_kernel(masks, first, gain_ref, gate_ref, up_ref, weight_ref, act_ref, square_ref, *refs):
    hidden_ref, pair_ref = refs[-2:]
    experts, model_width, hidden_width = gate_ref.shape
    rows = hidden_ref.shape[0]
    span = slice(first, first + rows)
    acts = [act_ref[e, span, :] for e in range(experts)]
    square = expand_part(masks, gain_ref, gate_ref, up_ref, refs[:-2], acts, square_ref[span, :1])
    scale = lax.rsqrt(square / model_width + EPSILON)
    firsts, seconds = places_of(weight_ref, span, experts)
    pair = [jnp.zeros((rows, hidden_width), F32)] * 2
    for e in range(experts):
        gate, up = acts[e][:, :hidden_width] * scale, acts[e][:, hidden_width:] * scale
        weight = weight_ref[span, ROPE + e : ROPE + e + 1]
        hidden = gate / (1.0 + jnp.exp(-gate)) * up * weight
        hidden_ref[:, e * hidden_width : (e + 1) * hidden_width] = hidden.astype(BF16)
        pair = [jnp.where(firsts[e], hidden, pair[0]), jnp.where(seconds[e], hidden, pair[1])]
    pair_ref[...] = jnp.concatenate(pair, axis=1).astype(BF16)


def own_kernel(down_ref, *refs):
    send_ref, keep_ref = refs[-2:]
    place = lax.axis_index("tp")
    quarter = send_ref.shape[1]
    hidden = jnp.concatenate([ref[...] for ref in refs[:-2]], axis=0)
    for ref, mask in ((send_ref, 1), (keep_ref, 0)):
        cols = pl.ds(pl.multiple_of((place ^ mask) * quarter, LANES), quarter)
        ref[...] = dot(hidden, down_ref[:, cols])


def join_kernel(count, first, weight_ref, part_send_ref, part_keep_ref, *refs):
    send_ref, keep_ref = refs[-2:]
    lows, highs, pairs = refs[:count], refs[count : 2 * count], refs[2 * count : -2]
    rows, quarter = send_ref.shape
    width = pairs[0].shape[1] // 2
    half_rows = lows[0].shape[0]
    experts = 2 * half_rows // width
    span = slice(first, first + rows)
    firsts, seconds = places_of(weight_ref, span, experts)
    send, keep = part_send_ref[span, :], part_keep_ref[span, :]
    core = lax.axis_index("tp") & 1
    for i in range(count):
        pair = pairs[i][...]
        zero = jnp.zeros((rows, width), F32)
        one, two = pair[:, :width].astype(F32), pair[:, width:].astype(F32)
        hidden = jnp.concatenate(
            [jnp.where(firsts[e], one, jnp.where(seconds[e], two, zero)) for e in range(experts)], axis=1
        ).astype(BF16)
        for bit in range(2):
            cols = pl.ds(pl.multiple_of((core ^ bit) * quarter, LANES), quarter)
            product = dot(hidden, jnp.concatenate([lows[i][:, cols], highs[i][:, cols]], axis=0))
            if bit:
                send = send + product
            else:
                keep = keep + product
    send_ref[...] = send.astype(BF16)
    keep_ref[...] = keep.astype(BF16)


def start_copies(sources, targets, semaphores):
    copies = [
        pltpu.make_async_copy(source, target, semaphores.at[i])
        for i, (source, target) in enumerate(zip(sources, targets))
    ]
    for copy in copies:
        copy.start()
    return copies


def call(kernel, outs, inputs, fetched=(), kept=(), cuts=(), mib=12):
    whole = lambda ref: ref
    pieces = [(a, whole, a.shape) for a in kept] + list(cuts)
    kept = [a for a, _, _ in pieces]
    n_in, n_fetched, n_kept, n_out = len(inputs), len(fetched), len(kept), len(outs)

    def wrapped(*refs):
        refs = list(refs)
        take = lambda n: [refs.pop(0) for _ in range(n)]
        ins, sources, kept_sources = take(n_in), take(n_fetched), take(n_kept)
        results, kept_results, held = take(n_out), take(n_kept), take(n_fetched)
        first = start_copies(sources, held, refs[0]) if n_fetched else []
        kept_sources = [piece[1](source) for piece, source in zip(pieces, kept_sources)]
        second = start_copies(kept_sources, kept_results, refs[-1]) if n_kept else []
        for copy in first:
            copy.wait()
        kernel(*ins, *held, *results)
        for copy in second:
            copy.wait()

    semaphores = [pltpu.SemaphoreType.DMA((n,)) for n in (n_fetched, n_kept) if n]
    return pl.pallas_call(
        wrapped,
        out_shape=list(outs) + [held_shape(dims, a.dtype) for a, _, dims in pieces],
        in_specs=[VMEM] * n_in + [HBM] * (n_fetched + n_kept),
        out_specs=[VMEM] * (n_out + n_kept),
        scratch_shapes=[pltpu.VMEM(a.shape, a.dtype) for a in fetched] + semaphores,
        compiler_params=pltpu.CompilerParams(vmem_limit_bytes=mib * 2**20),
    )(
        *(pltpu.with_memory_space_constraint(a, pltpu.VMEM) for a in inputs),
        *(pltpu.with_memory_space_constraint(a, pltpu.HBM) for a in (*fetched, *kept)),
    )


def shape(dims, dtype=BF16):
    return jax.ShapeDtypeStruct(dims, dtype)


def held_shape(dims, dtype=BF16):
    return pltpu.VMEM(dims, dtype)


def body(
    query_wide,
    query_narrow,
    latent,
    rope_key,
    latent_norm_weight,
    broad_key_lift,
    broad_value_lift,
    slim_key_lift,
    slim_value_lift,
    out_wide,
    out_narrow,
    resid,
    ffn_gain,
    group_route,
    expert_pair,
    group_prob,
    expert_prob,
    gate_weight,
    up_weight,
    down_weight,
):
    tokens, rank = latent.shape
    groups = lax.axis_size("sp")
    tp_size = lax.axis_size("tp")
    place = lax.axis_index("sp")
    half = tokens // 2
    capacity = 2 * tokens // groups
    slots = groups * capacity
    model_width = resid.shape[1]
    quarter = model_width // tp_size
    route = group_route[None, :]
    far_masks = list(range(2, tp_size, 2))
    down_rows = down_weight[0].reshape(-1, model_width)

    def resid_cut(ref):
        return ref.at[:, pl.ds(pl.multiple_of(lax.axis_index("tp") * quarter, LANES), quarter)]

    def down_cut(mask, which, ref):
        rows, width = down_rows.shape[0] // 2, 2 * quarter
        upper = (lax.axis_index("tp") ^ mask) >> 1
        return ref.at[pl.ds(which * rows, rows), pl.ds(pl.multiple_of(upper * width, LANES), width)]

    query_pos = place * tokens + jnp.arange(tokens, dtype=jnp.int32)
    table = angles(query_pos, ROPE).T
    packed = held_shape((half, rank + LANES))
    tables = [jnp.cos(table), jnp.sin(table)]
    own, rest = call(
        pack_kernel, [packed, packed], tables,
        [latent, rope_key.T, latent_norm_weight[None, :], route, expert_pair.T, group_prob[None, :], expert_prob.T],
        mib=4,
    )

    strides = list(range(groups - 2, 0, -2))
    got = []
    for k in strides:
        got.append(exchange(own, "sp", k))
    beside = exchange(own, "sp", 1)
    across = [beside[None], exchange(beside, "sp", strides[-1])[None]]
    across.append(exchange(jnp.stack(got[:-1]), "sp", 1))
    column = [own, jnp.stack(got)]
    column_rest = [rest, exchange(column[1], "tp", 1)]
    across = jnp.concatenate(across)
    across_rest = exchange(across, "tp", 1)
    first_masks = [0] + strides
    second_masks = [1, strides[-1] ^ 1] + [k ^ 1 for k in strides[:-1]]
    heads = query_wide.shape[1] // (PLAIN_WIDTH_WIDE + ROPE) + query_narrow.shape[1] // (PLAIN_WIDTH_SLIM + ROPE)
    queries, *weights = call(
        query_kernel, [held_shape((heads, tokens, 2 * LANES))], tables, [query_wide, query_narrow],
        [broad_key_lift, broad_value_lift, slim_key_lift, slim_value_lift, out_wide, out_narrow],
        [
            (down_rows, functools.partial(down_cut, mask, which), (down_rows.shape[0] // 2, 2 * quarter))
            for mask in far_masks
            for which in range(2)
        ],
        mib=4,
    )
    lifts, out_weights, down_cuts = weights[:4], weights[4:6], weights[6:]
    down_low = [exchange(down_cuts[2 * i], "tp", mask) for i, mask in enumerate(far_masks)]
    down_high = [exchange(down_cuts[2 * i + 1], "tp", mask) for i, mask in enumerate(far_masks)]
    state_shape = [held_shape((heads, tokens, LANES), F32)] * 3
    state = call(functools.partial(first_kernel, first_masks), state_shape, [queries, *lifts, *column, *column_rest])
    state += call(functools.partial(second_kernel, second_masks), state_shape, [queries, *lifts, across])
    pieces_shape = held_shape((tp_size // 2, tokens, quarter))
    send, att_w, att_n = call(
        functools.partial(third_kernel, second_masks),
        [pieces_shape, held_shape((tokens, out_wide.shape[0])), held_shape((tokens, out_narrow.shape[0]))],
        [queries, *lifts, *state, *out_weights, across_rest],
    )
    (keep,) = call(keep_kernel, [pieces_shape], [att_w, att_n, *out_weights], mib=4)
    slot_weights, hot, gate, up, down, gain, resid_cols = call(
        functools.partial(weights_kernel, first_masks + second_masks),
        [held_shape((slots, LANES), F32), held_shape((slots, tokens))],
        [route, *column, across, *column_rest, across_rest], [],
        [gate_weight[0], up_weight[0], down_rows, ffn_gain[None, :]],
        [(resid, resid_cut, (tokens, quarter))], mib=4,
    )

    received = exchange(send, "tp", 1)
    thin_rows = held_shape((tokens, quarter))
    stay, *sends = call(
        functools.partial(pair_kernel, far_masks), [thin_rows] * (1 + len(far_masks)), [keep, received], mib=4
    )
    came = [exchange(part, "tp", mask) for part, mask in zip(sends, far_masks)]
    stream_cols, placed = call(
        place_kernel, [thin_rows, held_shape((groups, capacity, quarter))],
        [resid_cols, hot, stay, *came], mib=4,
    )

    routed = lax.all_to_all(placed, "sp", split_axis=0, concat_axis=0, tiled=True)
    routed = routed.reshape(slots, quarter)
    part_rows = slots // 2
    far = []
    for first in (0, part_rows):
        far.append([exchange(routed[first : first + part_rows], "tp", mask) for mask in far_masks])
    near = exchange(routed, "tp", 1)
    experts, _, hidden_width = gate_weight[0].shape
    acts, square = call(
        functools.partial(near_kernel, [0, 1]),
        [held_shape((experts, slots, 2 * hidden_width), F32), held_shape((slots, LANES), F32)],
        [gain, gate, up, routed, near],
    )
    hidden, pairs = [], []
    for part in range(2):
        far_near = [exchange(rows, "tp", 1) for rows in far[part]]
        units, pair = call(
            functools.partial(far_kernel, far_masks + [m | 1 for m in far_masks], part * part_rows),
            [held_shape((part_rows, experts * hidden_width)), held_shape((part_rows, 2 * hidden_width))],
            [gain, gate, up, slot_weights, acts, square, *far[part], *far_near],
        )
        hidden.append(units)
        pairs.append([exchange(pair, "tp", mask) for mask in far_masks])
    wide = held_shape((slots, quarter), F32)
    thin = held_shape((part_rows, quarter))
    part_send, part_keep = call(own_kernel, [wide, wide], [down, *hidden])
    summed = []
    for part in range(2):
        send, keep = call(
            functools.partial(join_kernel, len(far_masks), part * part_rows), [thin, thin],
            [slot_weights, part_send, part_keep, *down_low, *down_high, *pairs[part]],
        )
        received = exchange(send, "tp", 1)
        summed.append((keep.astype(F32) + received.astype(F32)).astype(BF16))
    returned = lax.all_to_all(
        jnp.concatenate(summed).reshape(groups, capacity, quarter), "sp", split_axis=0, concat_axis=0, tiled=True
    )
    return call(final_kernel, [shape((tokens, quarter))], [stream_cols, returned, hot], mib=4)[0]


def solution(mesh):
    placed = (
        P("sp", "tp"),
        P("sp", "tp"),
        P("sp", None),
        P("sp", None),
        P(),
        P(None, "tp"),
        P(None, "tp"),
        P(None, "tp"),
        P(None, "tp"),
        P("tp", None),
        P("tp", None),
        P("sp", None),
        P(),
        P("sp"),
        P("sp", None),
        P("sp"),
        P("sp", None),
        P("sp", None, None, "tp"),
        P("sp", None, None, "tp"),
        P("sp", None, "tp", None),
    )
    return jax.shard_map(body, mesh=mesh, in_specs=placed, out_specs=P("sp", "tp"), check_vma=False)
```

```python
import functools

import jax
import jax.numpy as jnp
from jax import lax
from jax.experimental import pallas as pl
from jax.experimental.pallas import tpu as pltpu
from jax.sharding import PartitionSpec as P


PLAIN_WIDTH_WIDE = 128
PLAIN_WIDTH_SLIM = 64
ROPE = 64
VALUE_WIDTH_WIDE = 128
VALUE_WIDTH_SLIM = 64
EPG = 4
LANES = 128

ROPE_BASE = 10000.0
EPSILON = 1e-06
MASKED = -1e30


F32 = jnp.float32
BF16 = jnp.bfloat16
VMEM = pl.BlockSpec(memory_space=pltpu.VMEM)
HBM = pl.BlockSpec(memory_space=pltpu.HBM)


def angles(positions, width):
    frequency = 1.0 / ROPE_BASE ** (jnp.arange(0, width, 2).astype(F32) / width)
    return positions.astype(F32)[:, None] * frequency[None, :]


def turn(values, cosine, sine, axis):
    first_half, second = jnp.split(values, 2, axis=axis)
    return jnp.concatenate(
        [first_half * cosine - second * sine, second * cosine + first_half * sine], axis=axis
    )


def exchange(values, axis, mask):
    size = lax.axis_size(axis)
    return lax.ppermute(values, axis, [(i, i ^ mask) for i in range(size)])


def dot(a, b):
    return jnp.dot(a, b, preferred_element_type=F32)


def dot_t(a, b):
    return lax.dot_general(a, b, (((1,), (1,)), ((), ())), preferred_element_type=F32)


def iota(shape, dim):
    return lax.broadcasted_iota(jnp.int32, shape, dim)


def prefix_count(rows):
    size = rows.shape[1]
    upto = (iota((size, size), 0) <= iota((size, size), 1)).astype(BF16)
    return dot(rows.astype(BF16), upto)


def pack_kernel(
    cos_ref, sin_ref, latent_ref, rope_ref, gain_ref, route_ref, pair_ref, group_ref, prob_ref,
    half_ref, rest_ref,
):
    rank = latent_ref.shape[1]
    half = half_ref.shape[0]
    tokens = latent_ref.shape[0]
    odd = (lax.axis_index("tp") & 1) == 1
    widened = latent_ref[...].astype(F32)
    scale = lax.rsqrt(jnp.mean(widened * widened, axis=-1, keepdims=True) + EPSILON)
    normed = (widened * scale * gain_ref[...]).astype(BF16)
    turned = turn(rope_ref[...].astype(F32), cos_ref[...], sin_ref[...], 0)
    shares = group_ref[...] * prob_ref[...] / jnp.sum(prob_ref[...], axis=0, keepdims=True)
    rows = iota((LANES - ROPE, tokens), 0)
    meta = jnp.where(rows == EPG, route_ref[...].astype(F32), 0.0)
    for expert in range(EPG):
        chosen = jnp.sum(jnp.where(pair_ref[...] == expert, shares, 0.0), axis=0, keepdims=True)
        meta = jnp.where(rows == expert, chosen, meta)
    tail = jnp.concatenate([turned, meta], axis=0).T.astype(BF16)
    half_ref[:, :rank] = jnp.where(odd, normed[half:], normed[:half])
    half_ref[:, rank:] = jnp.where(odd, tail[half:], tail[:half])
    rest_ref[:, :rank] = jnp.where(odd, normed[:half], normed[half:])
    rest_ref[:, rank:] = jnp.where(odd, tail[:half], tail[half:])


def query_kernel(cos_ref, sin_ref, wide_ref, slim_ref, out_ref):
    tokens = wide_ref.shape[0]
    heads_w = wide_ref.shape[1] // (PLAIN_WIDTH_WIDE + ROPE)
    heads_n = slim_ref.shape[1] // (PLAIN_WIDTH_SLIM + ROPE)
    spare = jnp.zeros((tokens, LANES - ROPE), F32)
    cosine, sine = cos_ref[...].T, sin_ref[...].T
    for h in range(heads_w + heads_n):
        wide = h < heads_w
        plain = PLAIN_WIDTH_WIDE if wide else PLAIN_WIDTH_SLIM
        start = (h if wide else h - heads_w) * (plain + ROPE)
        part = (wide_ref if wide else slim_ref)[:, start : start + plain + ROPE].astype(F32)
        pieces = [part[:, :plain], turn(part[:, plain:], cosine, sine, 1), spare]
        if not wide:
            before = (h - heads_w) * plain
            after = heads_n * plain - before - plain
            if before:
                pieces = [jnp.zeros((tokens, before), F32)] + pieces
            if after:
                pieces = pieces[:-2] + [jnp.zeros((tokens, after), F32)] + pieces[-2:]
        out_ref[h] = jnp.concatenate(pieces, axis=1).astype(BF16)


def pieces_of(refs):
    return [
        piece
        for ref in refs
        for piece in ([ref[...]] if len(ref.shape) == 2 else [ref[i] for i in range(ref.shape[0])])
    ]


def attend_body(queries, pieces, masks, mine, kw_ref, vw_ref, kn_ref, vn_ref, state):
    heads_w = kw_ref.shape[1] // PLAIN_WIDTH_WIDE
    heads_n = kn_ref.shape[1] // PLAIN_WIDTH_SLIM
    half = pieces[0].shape[0]
    tokens = queries[0].shape[0]
    rank = kw_ref.shape[0]
    place = lax.axis_index("sp")
    core = lax.axis_index("tp") & 1
    shift = half.bit_length() - 1
    step = 8
    for start in range(0, len(pieces), step):
        group = pieces[start : start + step]
        rows = len(group) * half
        lat = jnp.concatenate(group, axis=0)
        flat = lat[:, :rank]
        rot = lat[:, rank:]
        key_w = dot(flat, kw_ref[...]).astype(BF16)
        key_n = dot(flat, kn_ref[...]).astype(BF16)
        val_w = dot(flat, vw_ref[...]).astype(BF16)
        val_n = dot(flat, vn_ref[...]).astype(BF16)
        lane = iota((1, rows), 1)
        index = lane >> shift
        mask = jnp.zeros_like(lane)
        offset = jnp.zeros_like(lane)
        for i in range(len(group)):
            mask = jnp.where(index == i, masks[start + i], mask)
            offset = jnp.where(index == i, core if mine[start + i] else 1 - core, offset)
        key_pos = ((place ^ mask) * 2 + offset) * half + (lane & (half - 1))
        visible = iota((tokens, 1), 0) + place * tokens >= key_pos
        scored = []
        for h in range(heads_w + heads_n):
            if h < heads_w:
                keys = key_w[:, h * PLAIN_WIDTH_WIDE : (h + 1) * PLAIN_WIDTH_WIDE]
                scale = (PLAIN_WIDTH_WIDE + ROPE) ** (-0.5)
            else:
                keys = key_n
                scale = (PLAIN_WIDTH_SLIM + ROPE) ** (-0.5)
            scores = dot_t(queries[h], jnp.concatenate([keys, rot], axis=1)) * scale
            scored.append(jnp.where(visible, scores, MASKED))
        peaks = [jnp.max(scores, axis=-1, keepdims=True) for scores in scored]
        if state is not None:
            peaks = [jnp.maximum(peak, state[h][0]) for h, peak in enumerate(peaks)]
        weighed = [jnp.exp(scores - peak) for scores, peak in zip(scored, peaks)]
        totals = [jnp.sum(weights, axis=-1, keepdims=True) for weights in weighed]
        accs = []
        for h, weights in enumerate(weighed):
            values = val_w[:, h * VALUE_WIDTH_WIDE : (h + 1) * VALUE_WIDTH_WIDE] if h < heads_w else val_n
            accs.append(dot(weights.astype(BF16), values))
        if state is not None:
            keeps = [jnp.exp(state[h][0] - peak) for h, peak in enumerate(peaks)]
            totals = [total + state[h][1] * keeps[h] for h, total in enumerate(totals)]
            accs = [acc + state[h][2] * keeps[h] for h, acc in enumerate(accs)]
        state = list(zip(peaks, totals, accs))
    return state


def store_state(state, refs):
    peak_ref, total_ref, acc_ref = refs
    for h, (peak, total, acc) in enumerate(state):
        peak_ref[h] = jnp.broadcast_to(peak, peak_ref.shape[1:])
        total_ref[h] = jnp.broadcast_to(total, total_ref.shape[1:])
        acc_ref[h] = acc


def merged(states):
    peak = functools.reduce(jnp.maximum, [part[0] for part in states])
    factors = [jnp.exp(part[0] - peak) for part in states]
    total = sum(part[1] * factor for part, factor in zip(states, factors))
    return sum(part[2] * factor for part, factor in zip(states, factors)) / total


def first_kernel(masks, q_ref, *refs):
    lifts, blocks = refs[:4], refs[4:-3]
    queries = [q_ref[h] for h in range(q_ref.shape[0])]
    mine = [True] * len(masks) + [False] * len(masks)
    store_state(attend_body(queries, pieces_of(blocks), masks * 2, mine, *lifts, None), refs[-3:])


def second_kernel(masks, q_ref, *refs):
    lifts, blocks = refs[:4], refs[4:-3]
    queries = [q_ref[h] for h in range(q_ref.shape[0])]
    state = attend_body(queries, pieces_of(blocks), masks, [True] * len(masks), *lifts, None)
    store_state(state, refs[-3:])


def third_kernel(masks, q_ref, *refs):
    lifts, state_refs, (ow_ref, on_ref), blocks = refs[:4], (refs[4:7], refs[7:10]), refs[10:12], refs[12:-3]
    send_ref, att_w_ref, att_n_ref = refs[-3:]
    queries = [q_ref[h] for h in range(q_ref.shape[0])]
    heads = len(queries)
    heads_w = lifts[0].shape[1] // PLAIN_WIDTH_WIDE
    state = attend_body(queries, pieces_of(blocks), masks, [False] * len(masks), *lifts, None)
    done = []
    for h, (peak, total, acc) in enumerate(state):
        fresh = (jnp.broadcast_to(peak, acc.shape), jnp.broadcast_to(total, acc.shape), acc)
        done.append(merged([fresh] + [tuple(ref[h] for ref in held) for held in state_refs]))
    att_w = jnp.concatenate(done[:heads_w], axis=1).astype(BF16)
    slim = done[heads_w]
    for h in range(1, heads - heads_w):
        lane = iota(slim.shape, 1)
        slim = jnp.where(lane >= h * VALUE_WIDTH_SLIM, done[heads_w + h], slim)
    att_n = slim.astype(BF16)
    att_w_ref[...] = att_w
    att_n_ref[...] = att_n
    project(att_w, att_n, ow_ref, on_ref, send_ref, 1 - (lax.axis_index("tp") & 1))


def project(att_w, att_n, ow_ref, on_ref, out_ref, bit):
    pieces, _, quarter = out_ref.shape
    for piece in range(pieces):
        cols = pl.ds(pl.multiple_of((2 * piece + bit) * quarter, LANES), quarter)
        out_ref[piece] = (dot(att_w, ow_ref[:, cols]) + dot(att_n, on_ref[:, cols])).astype(BF16)


def keep_kernel(att_w_ref, att_n_ref, ow_ref, on_ref, keep_ref):
    project(att_w_ref[...], att_n_ref[...], ow_ref, on_ref, keep_ref, lax.axis_index("tp") & 1)


def slots_of(route, groups, capacity):
    tokens = route.shape[1]
    member = (iota((groups, tokens), 0) == route).astype(F32)
    rank_of = jnp.sum(prefix_count(member) * member, axis=0, keepdims=True).astype(jnp.int32) - 1
    slot = route * capacity + rank_of
    return (iota((groups * capacity, tokens), 0) == slot).astype(BF16)


def weights_kernel(masks, route_ref, *refs):
    refs, hot_ref = refs[:-1], refs[-1]
    out_ref = refs[-1]
    count = (len(refs) - 1) // 2
    mine_all, other_all = pieces_of(refs[:count]), pieces_of(refs[count:-1])
    half, width = mine_all[0].shape
    place = lax.axis_index("sp")
    odd = (lax.axis_index("tp") & 1) == 1
    capacity = out_ref.shape[1] // len(mine_all)
    base = width - LANES
    hot_ref[...] = slots_of(route_ref[...], len(mine_all), capacity)
    for mask, mine, other in zip(masks, mine_all, other_all):
        mine, other = mine[:, base:], other[:, base:]
        data = jnp.concatenate(
            [jnp.where(odd, other, mine), jnp.where(odd, mine, other)], axis=0
        )
        route = data.astype(F32).T[ROPE + EPG : ROPE + EPG + 1]
        here = (route == place.astype(F32)).astype(F32)
        order = prefix_count(here) - 1.0
        hot = jnp.where((iota((capacity, 2 * half), 0).astype(F32) == order) & (here > 0), 1.0, 0.0)
        start = pl.multiple_of((place ^ mask) * capacity, capacity)
        weights = dot(hot.astype(BF16), data)
        for e in range(out_ref.shape[0]):
            column = weights[:, ROPE + e : ROPE + e + 1]
            out_ref[e, pl.ds(start, capacity), :] = jnp.broadcast_to(column, (capacity, out_ref.shape[2]))


def pair_kernel(masks, keep_ref, got_ref, stay_ref, *send_refs):
    upper = lax.axis_index("tp") >> 1
    for ref, mask in zip((stay_ref, *send_refs), [0] + masks):
        piece = upper ^ (mask >> 1)
        ref[...] = (keep_ref[piece].astype(F32) + got_ref[piece].astype(F32)).astype(BF16)


def place_kernel(resid_ref, hot_ref, *refs):
    stream_ref, placed_ref = refs[-2:]
    stream = resid_ref[...].astype(F32)
    for ref in refs[:-2]:
        stream = stream + ref[...].astype(F32)
    stream = stream.astype(BF16)
    stream_ref[...] = stream
    placed_ref[...] = dot(hot_ref[...], stream).astype(BF16).reshape(placed_ref.shape)


def final_kernel(stream_ref, back_ref, hot_ref, out_ref):
    groups, capacity, quarter = back_ref.shape
    rows = back_ref[...].reshape(groups * capacity, quarter)
    moe = lax.dot_general(hot_ref[...], rows, (((0,), (0,)), ((), ())), preferred_element_type=F32)
    out_ref[...] = (stream_ref[...].astype(F32) + moe).astype(BF16)


def expand_part(masks, gain_ref, gate_ref, up_ref, parts, acts, square):
    quarter = parts[0].shape[1]
    place = lax.axis_index("tp")
    for mask, part in zip(masks, parts):
        cols = pl.ds(pl.multiple_of((place ^ mask) * quarter, LANES), quarter)
        rows = part[...].astype(F32)
        square = square + jnp.sum(rows * rows, axis=-1, keepdims=True)
        scaled = (rows * gain_ref[:, cols]).astype(BF16)
        for e in range(len(acts)):
            both = jnp.concatenate([gate_ref[e, cols, :], up_ref[e, cols, :]], axis=1)
            acts[e] = acts[e] + dot(scaled, both)
    return square


def near_kernel(masks, gain_ref, gate_ref, up_ref, *refs):
    act_ref, square_ref = refs[-2:]
    acts = [0.0] * act_ref.shape[0]
    square = expand_part(masks, gain_ref, gate_ref, up_ref, refs[:-2], acts, 0.0)
    for e, act in enumerate(acts):
        act_ref[e] = act
    square_ref[...] = jnp.broadcast_to(square, square_ref.shape)


def places_of(weight_ref, span, experts):
    firsts, seconds = [], []
    seen = 0.0
    for e in range(experts):
        chosen = jnp.where(weight_ref[e, span, :] != 0.0, 1.0, 0.0)
        firsts.append((chosen > 0.0) & (seen == 0.0))
        seconds.append((chosen > 0.0) & (seen == 1.0))
        seen = seen + chosen
    return firsts, seconds


def far_kernel(masks, first, gain_ref, gate_ref, up_ref, weight_ref, act_ref, square_ref, *refs):
    hidden_ref, pair_ref = refs[-2:]
    experts, model_width, hidden_width = gate_ref.shape
    rows = hidden_ref.shape[0]
    span = slice(first, first + rows)
    acts = [act_ref[e, span, :] for e in range(experts)]
    square = expand_part(masks, gain_ref, gate_ref, up_ref, refs[:-2], acts, 0.0)
    square = square_ref[span, :] + jnp.broadcast_to(square, (rows, hidden_width))
    scale = lax.rsqrt(square / model_width + EPSILON)
    firsts, seconds = places_of(weight_ref, span, experts)
    pair = [jnp.zeros((rows, hidden_width), F32)] * 2
    for e in range(experts):
        gate, up = acts[e][:, :hidden_width] * scale, acts[e][:, hidden_width:] * scale
        hidden = gate / (1.0 + jnp.exp(-gate)) * up * weight_ref[e, span, :]
        hidden_ref[:, e * hidden_width : (e + 1) * hidden_width] = hidden.astype(BF16)
        pair = [jnp.where(firsts[e], hidden, pair[0]), jnp.where(seconds[e], hidden, pair[1])]
    pair_ref[...] = jnp.concatenate(pair, axis=1).astype(BF16)


def own_kernel(down_ref, *refs):
    send_ref, keep_ref = refs[-2:]
    place = lax.axis_index("tp")
    quarter = send_ref.shape[1]
    hidden = jnp.concatenate([ref[...] for ref in refs[:-2]], axis=0)
    for ref, mask in ((send_ref, 1), (keep_ref, 0)):
        cols = pl.ds(pl.multiple_of((place ^ mask) * quarter, LANES), quarter)
        ref[...] = dot(hidden, down_ref[:, cols])


def join_kernel(count, first, weight_ref, part_send_ref, part_keep_ref, *refs):
    send_ref, keep_ref = refs[-2:]
    lows, highs, pairs = refs[:count], refs[count : 2 * count], refs[2 * count : -2]
    rows, quarter = send_ref.shape
    width = pairs[0].shape[1] // 2
    half_rows = lows[0].shape[0]
    experts = 2 * half_rows // width
    span = slice(first, first + rows)
    firsts, seconds = places_of(weight_ref, span, experts)
    send, keep = part_send_ref[span, :], part_keep_ref[span, :]
    core = lax.axis_index("tp") & 1
    for i in range(count):
        pair = pairs[i][...]
        zero = jnp.zeros((rows, width), F32)
        one, two = pair[:, :width].astype(F32), pair[:, width:].astype(F32)
        hidden = jnp.concatenate(
            [jnp.where(firsts[e], one, jnp.where(seconds[e], two, zero)) for e in range(experts)], axis=1
        ).astype(BF16)
        for bit in range(2):
            cols = pl.ds(pl.multiple_of((core ^ bit) * quarter, LANES), quarter)
            product = dot(hidden, jnp.concatenate([lows[i][:, cols], highs[i][:, cols]], axis=0))
            if bit:
                send = send + product
            else:
                keep = keep + product
    send_ref[...] = send.astype(BF16)
    keep_ref[...] = keep.astype(BF16)


def start_copies(sources, targets, semaphores):
    copies = [
        pltpu.make_async_copy(source, target, semaphores.at[i])
        for i, (source, target) in enumerate(zip(sources, targets))
    ]
    for copy in copies:
        copy.start()
    return copies


def call(kernel, outs, inputs, fetched=(), kept=(), cuts=(), mib=12):
    whole = lambda ref: ref
    pieces = [(a, whole, a.shape) for a in kept] + list(cuts)
    kept = [a for a, _, _ in pieces]
    n_in, n_fetched, n_kept, n_out = len(inputs), len(fetched), len(kept), len(outs)

    def wrapped(*refs):
        refs = list(refs)
        take = lambda n: [refs.pop(0) for _ in range(n)]
        ins, sources, kept_sources = take(n_in), take(n_fetched), take(n_kept)
        results, kept_results, held = take(n_out), take(n_kept), take(n_fetched)
        first = start_copies(sources, held, refs[0]) if n_fetched else []
        kept_sources = [piece[1](source) for piece, source in zip(pieces, kept_sources)]
        second = start_copies(kept_sources, kept_results, refs[-1]) if n_kept else []
        for copy in first:
            copy.wait()
        kernel(*ins, *held, *results)
        for copy in second:
            copy.wait()

    semaphores = [pltpu.SemaphoreType.DMA((n,)) for n in (n_fetched, n_kept) if n]
    return pl.pallas_call(
        wrapped,
        out_shape=list(outs) + [held_shape(dims, a.dtype) for a, _, dims in pieces],
        in_specs=[VMEM] * n_in + [HBM] * (n_fetched + n_kept),
        out_specs=[VMEM] * (n_out + n_kept),
        scratch_shapes=[pltpu.VMEM(a.shape, a.dtype) for a in fetched] + semaphores,
        compiler_params=pltpu.CompilerParams(vmem_limit_bytes=mib * 2**20),
    )(
        *(pltpu.with_memory_space_constraint(a, pltpu.VMEM) for a in inputs),
        *(pltpu.with_memory_space_constraint(a, pltpu.HBM) for a in (*fetched, *kept)),
    )


def shape(dims, dtype=BF16):
    return jax.ShapeDtypeStruct(dims, dtype)


def held_shape(dims, dtype=BF16):
    return pltpu.VMEM(dims, dtype)


def body(
    query_wide,
    query_narrow,
    latent,
    rope_key,
    latent_norm_weight,
    broad_key_lift,
    broad_value_lift,
    slim_key_lift,
    slim_value_lift,
    out_wide,
    out_narrow,
    resid,
    ffn_gain,
    group_route,
    expert_pair,
    group_prob,
    expert_prob,
    gate_weight,
    up_weight,
    down_weight,
):
    tokens, rank = latent.shape
    groups = lax.axis_size("sp")
    tp_size = lax.axis_size("tp")
    place = lax.axis_index("sp")
    half = tokens // 2
    capacity = 2 * tokens // groups
    slots = groups * capacity
    model_width = resid.shape[1]
    quarter = model_width // tp_size
    route = group_route[None, :]
    far_masks = list(range(2, tp_size, 2))
    experts, _, hidden_width = gate_weight[0].shape
    down_rows = down_weight[0].reshape(-1, model_width)

    def resid_cut(ref):
        return ref.at[:, pl.ds(pl.multiple_of(lax.axis_index("tp") * quarter, LANES), quarter)]

    def down_cut(mask, which, ref):
        rows, width = down_rows.shape[0] // 2, 2 * quarter
        upper = (lax.axis_index("tp") ^ mask) >> 1
        return ref.at[pl.ds(which * rows, rows), pl.ds(pl.multiple_of(upper * width, LANES), width)]

    query_pos = place * tokens + jnp.arange(tokens, dtype=jnp.int32)
    table = angles(query_pos, ROPE).T
    packed = held_shape((half, rank + LANES))
    tables = [jnp.cos(table), jnp.sin(table)]
    own, rest = call(
        pack_kernel, [packed, packed], tables,
        [latent, rope_key.T, latent_norm_weight[None, :], route, expert_pair.T, group_prob[None, :], expert_prob.T],
        mib=4,
    )

    strides = list(range(groups - 2, 0, -2))
    got = []
    for k in strides:
        got.append(exchange(own, "sp", k))
    beside = exchange(own, "sp", 1)
    across = [beside[None], exchange(beside, "sp", strides[-1])[None]]
    across.append(exchange(jnp.stack(got[:-1]), "sp", 1))
    column = [own, jnp.stack(got)]
    column_rest = [rest, exchange(column[1], "tp", 1)]
    across = jnp.concatenate(across)
    across_rest = exchange(across, "tp", 1)
    first_masks = [0] + strides
    second_masks = [1, strides[-1] ^ 1] + [k ^ 1 for k in strides[:-1]]
    heads = query_wide.shape[1] // (PLAIN_WIDTH_WIDE + ROPE) + query_narrow.shape[1] // (PLAIN_WIDTH_SLIM + ROPE)
    queries, *weights = call(
        query_kernel, [held_shape((heads, tokens, 2 * LANES))], tables, [query_wide, query_narrow],
        [broad_key_lift, broad_value_lift, slim_key_lift, slim_value_lift, out_wide, out_narrow],
        [
            (down_rows, functools.partial(down_cut, mask, which), (down_rows.shape[0] // 2, 2 * quarter))
            for mask in far_masks
            for which in range(2)
        ],
        mib=4,
    )
    lifts, out_weights, down_cuts = weights[:4], weights[4:6], weights[6:]
    down_low = [exchange(down_cuts[2 * i], "tp", mask) for i, mask in enumerate(far_masks)]
    down_high = [exchange(down_cuts[2 * i + 1], "tp", mask) for i, mask in enumerate(far_masks)]
    state_shape = [held_shape((heads, tokens, LANES), F32)] * 3
    state = call(functools.partial(first_kernel, first_masks), state_shape, [queries, *lifts, *column, *column_rest])
    state += call(functools.partial(second_kernel, second_masks), state_shape, [queries, *lifts, across])
    pieces_shape = held_shape((tp_size // 2, tokens, quarter))
    send, att_w, att_n = call(
        functools.partial(third_kernel, second_masks),
        [pieces_shape, held_shape((tokens, out_wide.shape[0])), held_shape((tokens, out_narrow.shape[0]))],
        [queries, *lifts, *state, *out_weights, across_rest],
    )
    (keep,) = call(keep_kernel, [pieces_shape], [att_w, att_n, *out_weights], mib=4)
    slot_weights, hot, gate, up, down, gain, resid_cols = call(
        functools.partial(weights_kernel, first_masks + second_masks),
        [held_shape((experts, slots, hidden_width), F32), held_shape((slots, tokens))],
        [route, *column, across, *column_rest, across_rest], [],
        [gate_weight[0], up_weight[0], down_rows, ffn_gain[None, :]],
        [(resid, resid_cut, (tokens, quarter))], mib=4,
    )

    received = exchange(send, "tp", 1)
    thin_rows = held_shape((tokens, quarter))
    stay, *sends = call(
        functools.partial(pair_kernel, far_masks), [thin_rows] * (1 + len(far_masks)), [keep, received], mib=4
    )
    came = [exchange(part, "tp", mask) for part, mask in zip(sends, far_masks)]
    stream_cols, placed = call(
        place_kernel, [thin_rows, held_shape((groups, capacity, quarter))],
        [resid_cols, hot, stay, *came], mib=4,
    )

    routed = lax.all_to_all(placed, "sp", split_axis=0, concat_axis=0, tiled=True)
    routed = routed.reshape(slots, quarter)
    part_rows = slots // 2
    far = []
    for first in (0, part_rows):
        far.append([exchange(routed[first : first + part_rows], "tp", mask) for mask in far_masks])
    near = exchange(routed, "tp", 1)
    acts, square = call(
        functools.partial(near_kernel, [0, 1]),
        [held_shape((experts, slots, 2 * hidden_width), F32), held_shape((slots, hidden_width), F32)],
        [gain, gate, up, routed, near],
    )
    hidden, pairs = [], []
    for part in range(2):
        far_near = [exchange(rows, "tp", 1) for rows in far[part]]
        units, pair = call(
            functools.partial(far_kernel, far_masks + [m | 1 for m in far_masks], part * part_rows),
            [held_shape((part_rows, experts * hidden_width)), held_shape((part_rows, 2 * hidden_width))],
            [gain, gate, up, slot_weights, acts, square, *far[part], *far_near],
        )
        hidden.append(units)
        pairs.append([exchange(pair, "tp", mask) for mask in far_masks])
    wide = held_shape((slots, quarter), F32)
    thin = held_shape((part_rows, quarter))
    part_send, part_keep = call(own_kernel, [wide, wide], [down, *hidden])
    summed = []
    for part in range(2):
        send, keep = call(
            functools.partial(join_kernel, len(far_masks), part * part_rows), [thin, thin],
            [slot_weights, part_send, part_keep, *down_low, *down_high, *pairs[part]],
        )
        received = exchange(send, "tp", 1)
        summed.append((keep.astype(F32) + received.astype(F32)).astype(BF16))
    returned = lax.all_to_all(
        jnp.concatenate(summed).reshape(groups, capacity, quarter), "sp", split_axis=0, concat_axis=0, tiled=True
    )
    return call(final_kernel, [shape((tokens, quarter))], [stream_cols, returned, hot], mib=4)[0]


def solution(mesh):
    placed = (
        P("sp", "tp"),
        P("sp", "tp"),
        P("sp", None),
        P("sp", None),
        P(),
        P(None, "tp"),
        P(None, "tp"),
        P(None, "tp"),
        P(None, "tp"),
        P("tp", None),
        P("tp", None),
        P("sp", None),
        P(),
        P("sp"),
        P("sp", None),
        P("sp"),
        P("sp", None),
        P("sp", None, None, "tp"),
        P("sp", None, None, "tp"),
        P("sp", None, "tp", None),
    )
    return jax.shard_map(body, mesh=mesh, in_specs=placed, out_specs=P("sp", "tp"), check_vma=False)
```
